128 devices in a mesh: sp: 32 (over z, y, core), tp: 4 (over x).
Axes of the slice: x: 4, y: 4, z: 4, core: 2. Of those that a mesh axis runs over, the one named last changes fastest.
Arguments:
- queries: bfloat16 [16384, 2048], P('sp', 'tp'), may hold values from -6 to 6
- keys: bfloat16 [16384, 2048], P('sp', 'tp'), may hold values from -6 to 6
- values: bfloat16 [16384, 2048], P('sp', 'tp'), may hold values from -6 to 6
- output_gate_logits: bfloat16 [16384, 2048], P('sp', 'tp'), may hold values from -6 to 6
- decay_gate_logits: float32 [2, 16384, 16], P(None, 'sp', 'tp'), may hold values from -6 to 6
- write_strength_logits: float32 [2, 16384, 16], P(None, 'sp', 'tp'), may hold values from -7 to -4
- extra_log_decay: float32 [2, 16384, 16], P(None, 'sp', 'tp'), may hold values from -2.1 to 0
- head_decay_rate: float32 [2, 16], P(None, 'tp'), may hold values from 0 to 0.04
- head_norm_gain: bfloat16 [128], replicated, may hold values from 0.099609375 to 1.8984375
- output_weight: bfloat16 [2048, 4096], P('tp'), may hold values from -0.125 to 0.125
- residual: bfloat16 [16384, 4096], P(('sp', 'tp')), may hold values from -6 to 6
- expert_norm_gain: bfloat16 [4096], replicated, may hold values from 0.099609375 to 1.8984375
- selected_experts: int32 [16384, 2], P(('sp', 'tp')), may hold values from 0 to 31, all different within a row; in each aligned block of 128 rows (0 to 127, 128 to 255, ...) at most 12 rows name the same one
- router_chosen_scores: float32 [16384, 2], P(('sp', 'tp')), may hold values from -6 to 6
- gate_up_weight: bfloat16 [32, 4096, 1536], P('sp', None, 'tp'), may hold values from -0.75 to 0.75
- linear_up_weight: bfloat16 [32, 4096, 1536], P('sp', None, 'tp'), may hold values from -0.375 to 0.375
- down_weight: bfloat16 [32, 1536, 4096], P('sp', 'tp'), may hold values from -0.009765625 to 0.009765625
Outputs:
- block_out: bfloat16 [16384, 4096], P(('sp', 'tp'))
The draws below stay inside these ranges and needn't reach their ends.
Inputs may be any that keep to these rules, and one draw needn't show every extreme that they name: `selected_experts`: each row names 2 different experts. In each aligned block of rows that one device holds, no expert is named by more than 12 rows, and in every draw some expert is named by exactly 12 rows of some block.
All inputs are finite; a program needn't handle non-finite values.
Results may differ from the reference program's by a relative error of at most 0.02.
Values may be sent and summed in bfloat16 or wider, within the bound.
A program may use at most 128 MiB of HBM per device.

```python
import math
import jax
import jax.numpy as jnp
import numpy as np
from jax import lax

D = 4096
HEADS = 16
HEAD_DIM = 128
WIDTH = 2048
FF = 1536
TOPK = 2
EXPERTS = 32
BLOCK = 128
TOK_DEV = 512
SEQ = 16384
CAP = 12
N_SP = 32
N_TP = 4


def draw_head_decay_rate(key, part):
    chooser = jax.random.uniform(jax.random.fold_in(key, 11), (2, HEADS), jnp.float32)
    slow_rate = jnp.exp(jax.random.uniform(jax.random.fold_in(key, 12), (2, HEADS), jnp.float32, math.log(0.1), math.log(0.5))) / SEQ
    fast_rate = jnp.exp(jax.random.uniform(jax.random.fold_in(key, 13), (2, HEADS), jnp.float32, math.log(1.0 / 90.0), math.log(1.0 / 27.0)))
    slow_share = 0.5
    return jnp.where(chooser < slow_share, slow_rate, fast_rate).astype(jnp.float32)


def draw_decay_gate_logits(key, part):
    nblocks = SEQ // TOK_DEV
    offset = jax.random.uniform(jax.random.fold_in(key, 21), (2, nblocks, HEADS), jnp.float32, -1.0, 1.5)
    offset_full = jnp.repeat(offset, TOK_DEV, axis=1)
    noise = jnp.clip(jax.random.normal(jax.random.fold_in(key, 23), (2, SEQ, HEADS), jnp.float32), -4.0, 4.0)
    return (offset_full + noise).astype(jnp.float32)


def draw_extra_log_decay(key, part):
    spots = jax.random.randint(jax.random.fold_in(key, 31), (2, 3, HEADS), 0, SEQ)
    depth = jnp.log(jax.random.uniform(jax.random.fold_in(key, 32), (2, 3, HEADS), jnp.float32, 0.5, 0.8))
    position = jnp.arange(SEQ)[None, :, None, None]
    hits = position == spots[:, None, :, :]
    return jnp.sum(jnp.where(hits, depth[:, None, :, :], 0.0), axis=2).astype(jnp.float32)


def level_of(stream_key, dims, split, least, largest):
    level = 1.0
    for axis_at, shards_of in split:
        heights = jax.random.uniform(jax.random.fold_in(jax.random.fold_in(stream_key, 6), axis_at), (shards_of,), jnp.float32, least / len(split), largest / len(split))
        level = level * jnp.repeat(jnp.exp(heights), dims[axis_at] // shards_of).reshape((-1,) + (1,) * (len(dims) - 1 - axis_at))
    return level


def assign_block(key, own, number, rows, amount, top, limit, skew):
    order = jax.random.permutation(key, amount)
    crowded, usual = load_shares(amount, rows * top, limit, skew, True), load_shares(amount, rows * top, limit, skew, False)
    places = jnp.arange(amount)

    def named(lengths, offset_by):
        used = int((lengths > 0).sum())
        fixed = max(1, used // 4)
        moved = fixed + (places - fixed + offset_by * (used - fixed)) % max(1, amount - fixed)
        return jnp.zeros((amount,), jnp.int32).at[order[jnp.where(places < fixed, places, moved)]].set(jnp.asarray(lengths, jnp.int32))

    lengths = jnp.where(number % 4 == 0, named(crowded, number // 4), named(usual, number - number // 4 - 1))
    mixed = jax.random.permutation(jax.random.fold_in(own, 3), amount)
    giver, taker = mixed[0:amount // 2 * 2:2], mixed[1:amount // 2 * 2:2]
    slack = jnp.minimum(lengths[giver] - 1, limit - lengths[taker]) // 2
    slack = jnp.where((giver == order[0]) | (taker == order[0]) | (lengths[taker] == 0), 0, jnp.maximum(slack, 0))
    moved = jax.random.randint(jax.random.fold_in(own, 4), (amount // 2,), 0, 1 << 20) % (slack + 1)
    lengths = lengths.at[giver].add(-moved).at[taker].add(moved)
    members = jnp.searchsorted(jnp.cumsum(lengths), jnp.arange(rows * top), side="right").astype(jnp.int32)
    table = members.reshape(top, rows).T
    table = table[jax.random.permutation(jax.random.fold_in(own, 1), rows)]
    offset_by = jax.random.randint(jax.random.fold_in(own, 2), (rows, 1), 0, top)
    return jnp.take_along_axis(table, (jnp.arange(top)[None, :] + offset_by) % top, axis=1)


def load_shares(number_of, total, most, lean, full):
    loads = [(1 << 20) // math.isqrt(grade ** lean) + 1 for grade in range(1, number_of + 1)]
    largest = most if full else min(most, max(-(-total // number_of), total * loads[0] // sum(loads)))
    least = 1 if total - largest >= number_of - 1 else 0
    counts, rest = [largest] + [least] * (number_of - 1), total - largest - least * (number_of - 1)
    while rest > 0:
        candidates = [i for i in range(1, number_of) if counts[i] < largest] or [i for i in range(1, number_of) if counts[i] < most]
        mass, left = sum([loads[i] for i in candidates]), rest
        for i in candidates:
            addition = min(most - counts[i], max(1, left * loads[i] // mass), rest)
            counts[i] = counts[i] + addition
            rest = rest - addition
    return np.array(counts)


def centred(key, shape, scale, reach, cuts=(), kind=jnp.bfloat16):
    entries = scale * jax.random.normal(key, shape, jnp.float32)
    if cuts:
        entries = entries * level_of(key, shape, cuts, -0.22, 0.18)
    return jnp.clip(entries, -reach, reach).astype(kind)


def setup_inputs(seed: int = 0) -> dict:
    key_of = jax.random.split(jax.random.key(seed), 18)
    queries = centred(key_of[0], (SEQ, WIDTH), 1.0, 6.0, ((0, 32), (1, 4)))
    keys = centred(key_of[1], (SEQ, WIDTH), 1.0, 6.0, ((0, 32), (1, 4)))
    values = centred(key_of[2], (SEQ, WIDTH), 1.0, 6.0, ((0, 32), (1, 4)))
    output_gate_logits = centred(key_of[3], (SEQ, WIDTH), 1.0, 6.0, ((0, 32), (1, 4)))
    decay_gate_logits = draw_decay_gate_logits(jax.random.fold_in(key_of[17], 71), 0)
    write_strength_logits = jnp.clip(-7.0 + 3.0 * jax.random.uniform(key_of[5], (2, SEQ, HEADS), jnp.float32) ** level_of(key_of[5], (2, SEQ, HEADS), ((1, 32), (2, 4)), -0.2, 0.2), -7.0, -4.0)
    extra_log_decay = draw_extra_log_decay(jax.random.fold_in(key_of[17], 71), 0)
    head_decay_rate = draw_head_decay_rate(jax.random.fold_in(key_of[17], 71), 0)
    head_norm_gain = jnp.clip(1.0 + 0.18 * jax.random.normal(key_of[8], (HEAD_DIM,), jnp.float32), 0.099609375, 1.8984375).astype(jnp.bfloat16)
    output_weight = centred(key_of[9], (WIDTH, D), WIDTH ** -0.5, 0.125, ((0, 4),))
    residual = centred(key_of[10], (SEQ, D), 1.0, 6.0, ((0, 128),))
    expert_norm_gain = jnp.clip(1.0 + 0.18 * jax.random.normal(key_of[11], (D,), jnp.float32), 0.099609375, 1.8984375).astype(jnp.bfloat16)
    selected_experts_keys = jax.random.split(jax.random.fold_in(key_of[12], 1), SEQ // (TOK_DEV // N_TP))
    selected_experts_turns = jax.random.permutation(jax.random.fold_in(key_of[12], 3), SEQ // (TOK_DEV // N_TP))
    selected_experts = jax.vmap(lambda own, number: assign_block(jax.random.fold_in(key_of[12], 2), own, number, TOK_DEV // N_TP, EXPERTS, TOPK, CAP, 2))(selected_experts_keys, selected_experts_turns).reshape((SEQ, TOPK))
    router_chosen_scores = centred(key_of[13], (SEQ, TOPK), 1.0, 6.0, ((0, 128),), jnp.float32)
    gate_up_weight = centred(key_of[14], (EXPERTS, D, FF), (D // 64) ** -0.5, 0.75, ((0, 32), (2, 4)))
    linear_up_weight = centred(key_of[15], (EXPERTS, D, FF), (D // 16) ** -0.5, 0.375, ((0, 32), (2, 4)))
    down_weight = centred(key_of[16], (EXPERTS, FF, D), (FF * 256) ** -0.5, 0.009765625, ((0, 32), (1, 4)))
    return {"queries": queries, "keys": keys, "values": values, "output_gate_logits": output_gate_logits, "decay_gate_logits": decay_gate_logits, "write_strength_logits": write_strength_logits, "extra_log_decay": extra_log_decay, "head_decay_rate": head_decay_rate, "head_norm_gain": head_norm_gain, "output_weight": output_weight, "residual": residual, "expert_norm_gain": expert_norm_gain, "selected_experts": selected_experts, "router_chosen_scores": router_chosen_scores, "gate_up_weight": gate_up_weight, "linear_up_weight": linear_up_weight, "down_weight": down_weight}


highest = lax.Precision.HIGHEST

def unit_rows(tensor):
    return tensor * lax.rsqrt(lax.optimization_barrier(jnp.sum(tensor * tensor, axis=-1, keepdims=True)) + 1e-06)

def prepare(query_blk, key_blk, value_blk, log_blk, beta_blk):
    cumulative = jnp.cumsum(log_blk, axis=-1)
    position = jnp.arange(log_blk.shape[-1])
    inclusive = position[:, None] >= position[None, :]
    strict = position[:, None] > position[None, :]
    log_gap = cumulative[..., :, None] - cumulative[..., None, :]
    decay_mat = jnp.where(inclusive, jnp.exp(jnp.where(inclusive, log_gap, 0.0)), 0.0)
    key_beta = key_blk * beta_blk[..., None]
    lower_part = jnp.where(strict, jnp.einsum('hnid,hnjd->hnij', key_beta, key_blk, precision=highest) * decay_mat, 0.0)
    lower_mat = lower_part + jnp.eye(log_blk.shape[-1], dtype=jnp.float32)
    corrected = lax.linalg.triangular_solve(lower_mat, value_blk * beta_blk[..., None], left_side=True, lower=True, unit_diagonal=True)
    weighted = lax.linalg.triangular_solve(lower_mat, key_beta * jnp.exp(cumulative)[..., None], left_side=True, lower=True, unit_diagonal=True)
    block_decay = cumulative[..., -1]
    key_end = key_blk * jnp.exp(block_decay[..., None] - cumulative)[..., None]
    query_decay = query_blk * jnp.exp(cumulative)[..., None]
    query_key = jnp.where(inclusive, jnp.einsum('hnid,hnjd->hnij', query_blk, key_blk, precision=highest) * decay_mat, 0.0)
    return (corrected, weighted, key_end, block_decay, query_decay, query_key)

def block_sweep(parts, state, transfer, track_map, emit_out):
    by_block = tuple((jnp.moveaxis(tensor, 1, 0) for tensor in parts))

    def block_step(carried, block_parts):
        state_now, transfer_now = carried
        corrected, weighted, key_end, block_decay, query_decay, query_key = block_parts
        carry_scale = jnp.exp(block_decay)[:, None, None]
        fresh_values = corrected - jnp.einsum('hid,hde->hie', weighted, state_now, precision=highest)
        state_next = carry_scale * state_now + jnp.einsum('hid,hie->hde', key_end, fresh_values, precision=highest)
        emitted = ()
        if emit_out:
            emitted = emitted + (jnp.einsum('hid,hde->hie', query_decay, state_now, precision=highest) + jnp.einsum('hij,hje->hie', query_key, fresh_values, precision=highest),)
        transfer_next = transfer_now
        if track_map:
            moved_map = jnp.einsum('hid,hde->hie', weighted, transfer_now, precision=highest)
            transfer_next = carry_scale * transfer_now - jnp.einsum('hid,hie->hde', key_end, moved_map, precision=highest)
            if emit_out:
                emitted = emitted + (jnp.einsum('hid,hde->hie', query_decay, transfer_now, precision=highest) - jnp.einsum('hij,hje->hie', query_key, moved_map, precision=highest),)
        return ((state_next, transfer_next), emitted)
    return lax.scan(block_step, (state, transfer), by_block)

def one_direction(query_heads, key_heads, value_heads, log_heads, beta_heads):
    head_count = query_heads.shape[0]
    nblocks = query_heads.shape[1] // BLOCK

    def to_blocks(tensor):
        return tensor.reshape((head_count, nblocks, BLOCK) + tensor.shape[2:])
    parts = prepare(to_blocks(query_heads), to_blocks(key_heads), to_blocks(value_heads), to_blocks(log_heads), to_blocks(beta_heads))
    zero_state = jnp.zeros((head_count, HEAD_DIM, HEAD_DIM), jnp.float32)
    finals, emitted = block_sweep(parts, zero_state, zero_state, False, True)
    return jnp.moveaxis(emitted[0], 0, 1).reshape(head_count, -1, HEAD_DIM)

def reference(queries, keys, values, output_gate_logits, decay_gate_logits, write_strength_logits, extra_log_decay, head_decay_rate, head_norm_gain, output_weight, residual, expert_norm_gain, selected_experts, router_chosen_scores, gate_up_weight, linear_up_weight, down_weight):
    seq_len = queries.shape[0]

    def split_heads(tensor):
        return tensor.astype(jnp.float32).reshape(seq_len, HEADS, HEAD_DIM).transpose(1, 0, 2)

    def reverse_tokens(tensor):
        return jnp.flip(tensor, axis=1)
    query_heads = unit_rows(split_heads(queries)) * HEAD_DIM ** (-0.5)
    key_heads = unit_rows(split_heads(keys))
    value_heads = split_heads(values)
    decay_logarithm = (-head_decay_rate[:, None, :] * jax.nn.softplus(decay_gate_logits) + extra_log_decay).transpose(0, 2, 1)
    beta_gate = jax.nn.sigmoid(write_strength_logits).transpose(0, 2, 1)
    forward_out = one_direction(query_heads, key_heads, value_heads, decay_logarithm[0], beta_gate[0])
    backward_out = reverse_tokens(one_direction(reverse_tokens(query_heads), reverse_tokens(key_heads), reverse_tokens(value_heads), reverse_tokens(decay_logarithm[1]), reverse_tokens(beta_gate[1])))
    summed_heads = (forward_out + backward_out).transpose(1, 0, 2)
    scaled_heads = summed_heads * lax.rsqrt(lax.optimization_barrier(jnp.mean(summed_heads * summed_heads, axis=-1, keepdims=True)) + 1e-06) * head_norm_gain.astype(jnp.float32)
    gate_heads = output_gate_logits.astype(jnp.float32).reshape(seq_len, HEADS, HEAD_DIM)
    head_mix = (scaled_heads * jax.nn.silu(gate_heads)).reshape(seq_len, WIDTH).astype(jnp.bfloat16)
    head_piece = WIDTH // N_TP
    mix_sum = jnp.zeros((seq_len, D), jnp.float32)
    for piece_idx in range(N_TP):
        partial_sum = jnp.dot(head_mix[:, piece_idx * head_piece:(piece_idx + 1) * head_piece].astype(jnp.float32), output_weight[piece_idx * head_piece:(piece_idx + 1) * head_piece].astype(jnp.float32), preferred_element_type=jnp.float32).astype(jnp.bfloat16)
        partial_sum = lax.optimization_barrier(partial_sum)
        mix_sum = mix_sum + partial_sum.astype(jnp.float32)
    stream = (residual.astype(jnp.float32) + mix_sum).astype(jnp.bfloat16)
    stream_wide = stream.astype(jnp.float32)
    normed = (stream_wide * lax.rsqrt(lax.optimization_barrier(jnp.mean(stream_wide * stream_wide, axis=-1, keepdims=True)) + 1e-06) * expert_norm_gain.astype(jnp.float32)).astype(jnp.bfloat16)
    route_exp = jnp.exp(router_chosen_scores)
    route_weight = route_exp / lax.optimization_barrier(jnp.sum(route_exp, axis=-1, keepdims=True))
    flat_experts = selected_experts.reshape(-1).astype(jnp.int32)
    flat_weight = route_weight.reshape(-1)
    most_rows = CAP * N_SP * N_TP
    ff_piece = FF // N_TP

    def one_expert(total, expert):
        member = flat_experts == expert
        member_count = jnp.sum(member.astype(jnp.int32))
        where_rows = jnp.nonzero(member, size=most_rows, fill_value=0)[0].astype(jnp.int32)
        live_rows = jnp.arange(most_rows, dtype=jnp.int32) < member_count
        token_rows = (where_rows // TOPK).astype(jnp.int32)
        chosen = normed[token_rows]
        gate_pre = jnp.dot(chosen.astype(jnp.float32), gate_up_weight[expert].astype(jnp.float32), preferred_element_type=jnp.float32)
        linear_pre = jnp.dot(chosen.astype(jnp.float32), linear_up_weight[expert].astype(jnp.float32), preferred_element_type=jnp.float32)
        clipped = jnp.minimum(gate_pre, 7.0)
        hidden_act = (clipped * jax.nn.sigmoid(1.702 * clipped) * (jnp.clip(linear_pre, -7.0, 7.0) + 1.0)).astype(jnp.bfloat16)
        down_rows = down_weight[expert]
        expert_sum = jnp.zeros((most_rows, D), jnp.float32)
        for piece_idx in range(N_TP):
            piece_out = jnp.dot(hidden_act[:, piece_idx * ff_piece:(piece_idx + 1) * ff_piece].astype(jnp.float32), down_rows[piece_idx * ff_piece:(piece_idx + 1) * ff_piece].astype(jnp.float32), preferred_element_type=jnp.float32).astype(jnp.bfloat16)
            piece_out = lax.optimization_barrier(piece_out)
            expert_sum = expert_sum + piece_out.astype(jnp.float32)
        expert_out = lax.optimization_barrier(expert_sum.astype(jnp.bfloat16)).astype(jnp.float32)
        row_weight = jnp.where(live_rows, flat_weight[where_rows], 0.0)
        return (total.at[token_rows].add(expert_out * row_weight[:, None]), None)
    combined, finals = lax.scan(one_expert, jnp.zeros((seq_len, D), jnp.float32), jnp.arange(EXPERTS, dtype=jnp.int32))
    return (stream.astype(jnp.float32) + combined).astype(jnp.bfloat16)
```

```python
import jax
import jax.numpy as jnp
from jax import lax
from jax.experimental import pallas as pl
from jax.experimental.pallas import tpu as pltpu
from jax.sharding import Mesh
from jax.sharding import PartitionSpec as P

HEAD_DIM = 128
TOPK = 2
BLOCK = 128
SP = ("sp_0", "sp_1", "sp_2")
SP_TP = ("sp_0", "sp_1", "sp_2", "tp")
ARB = pltpu.CompilerParams(dimension_semantics=("arbitrary",), vmem_limit_bytes=48 * 1024 * 1024)
MESH = pl.DeviceIdType.MESH
NBLK = 4
f32 = jnp.float32
bf16 = jnp.bfloat16


def mm(a, b):
    return jnp.dot(a, b, preferred_element_type=f32)


def local_kernel(q_ref, k_ref, v_ref, ld_ref, bt_ref, out_ref, qeff_ref, blk_ref, comp_ref):
    n = BLOCK
    row = lax.broadcasted_iota(jnp.int32, (n, n), 0)
    col = lax.broadcasted_iota(jnp.int32, (n, n), 1)
    upper = (row <= col).astype(f32)
    lower = (row >= col).astype(f32)
    eye = (row == col).astype(f32)
    ld = ld_ref[0]
    highest = lax.Precision.HIGHEST
    run_f = jnp.dot(ld, upper, precision=highest, preferred_element_type=f32)
    run_b = jnp.dot(ld, lower, precision=highest, preferred_element_type=f32)
    which = lax.broadcasted_iota(jnp.int32, (2 * NBLK, n), 0)
    cum_rows = jnp.where(which < NBLK, run_f, run_b)
    cum_cols = jnp.transpose(cum_rows)
    beta_cols = jnp.transpose(bt_ref[0])
    chains = [(d, b) for d in range(2) for b in range(NBLK)]
    grams, k_un, v_un, q_un, kt_un = [], [], [], [], []
    for b in range(NBLK):
        rows = pl.ds(b * n, n)
        q = q_ref[rows, :].astype(f32)
        k = k_ref[rows, :].astype(f32)
        q = q * lax.rsqrt(jnp.sum(q * q, axis=-1, keepdims=True) + 1e-06) * HEAD_DIM ** (-0.5)
        k = k * lax.rsqrt(jnp.sum(k * k, axis=-1, keepdims=True) + 1e-06)
        kt = jnp.transpose(k).astype(bf16)
        grams.append((mm(k.astype(bf16), kt), mm(q.astype(bf16), kt)))
        q_un.append(q)
        k_un.append(k)
        kt_un.append(kt)
        v_un.append(v_ref[rows, :].astype(f32))
    low, attn, sums, pows = {}, {}, {}, {}
    for d, b in chains:
        i = d * NBLK + b
        gap = cum_cols[:, i : i + 1] - cum_rows[i : i + 1, :]
        keep = row >= col if d == 0 else row <= col
        decay = jnp.exp(jnp.where(keep, gap, -1e30))
        attn[d, b] = (grams[b][1] * decay).astype(bf16)
        strict = row > col if d == 0 else row < col
        low = jnp.where(strict, grams[b][0] * decay, 0.0) * beta_cols[:, i : i + 1]
        sums[d, b] = eye - low
        pows[d, b] = low.astype(bf16)
    for c in chains:
        pows[c] = mm(pows[c], pows[c]).astype(bf16)
    for step in range(5):
        for c in chains:
            both = mm(jnp.concatenate([sums[c].astype(bf16), pows[c]], axis=0), pows[c])
            sums[c] = sums[c] + both[:n]
            pows[c] = both[n:].astype(bf16)
    for c in chains:
        sums[c] = sums[c] + mm(sums[c].astype(bf16), pows[c])
    fresh, maps = {}, {}
    for d, b in chains:
        i = d * NBLK + b
        cc = cum_cols[:, i : i + 1]
        bt = beta_cols[:, i : i + 1]
        right = jnp.concatenate([v_un[b] * bt, k_un[b] * (-bt * jnp.exp(cc))], axis=1)
        fresh[d, b] = mm(sums[d, b].astype(bf16), right.astype(bf16))
    for d, b in chains:
        i = d * NBLK + b
        cc = cum_cols[:, i : i + 1]
        last = n - 1 if d == 0 else 0
        total = cum_rows[i : i + 1, last : last + 1]
        ended = (fresh[d, b] * jnp.exp(total - cc)).astype(bf16)
        step_map = mm(kt_un[b], ended) + jnp.concatenate(
            [jnp.zeros((n, n), f32), eye * jnp.exp(total)], axis=1
        )
        maps[d, b] = step_map
        blk_ref[0, i] = step_map.astype(bf16)
    for b in range(NBLK):
        rows = pl.ds(b * n, n)
        locals_, effs = [], []
        for d in range(2):
            i = d * NBLK + b
            given = mm(attn[d, b], fresh[d, b].astype(bf16))
            locals_.append(given[:, :n])
            effs.append(given[:, n:] + q_un[b] * jnp.exp(cum_cols[:, i : i + 1]))
        out_ref[rows, :] = locals_[0] + locals_[1]
        qeff_ref[0, rows, :] = jnp.concatenate(effs, axis=1).astype(bf16)

    def after(later, earlier):
        moved = mm(later[:, n:].astype(bf16), earlier.astype(bf16))
        return jnp.concatenate([moved[:, :n] + later[:, :n], moved[:, n:]], axis=1)

    for d in range(2):
        order = range(NBLK) if d == 0 else range(NBLK - 1, -1, -1)
        first, second, third, fourth = [maps[d, b] for b in order]
        comp_ref[0, d] = after(after(fourth, third), after(second, first)).astype(bf16)


def local_pass(queries, keys, values, log_decay, beta, heads):
    tok = queries.shape[0]
    n = BLOCK
    columns = pl.BlockSpec((tok, n), lambda h: (0, h))
    small = pl.BlockSpec((1, 2 * NBLK, n), lambda h: (h, 0, 0))
    return pl.pallas_call(
        local_kernel,
        grid=(heads,),
        in_specs=[columns, columns, columns, small, small],
        out_specs=[
            columns,
            pl.BlockSpec((1, tok, 2 * n), lambda h: (h, 0, 0)),
            pl.BlockSpec((1, 2 * NBLK, n, 2 * n), lambda h: (h, 0, 0, 0)),
            pl.BlockSpec((1, 2, n, 2 * n), lambda h: (h, 0, 0, 0)),
        ],
        out_shape=[
            jax.ShapeDtypeStruct((tok, heads * n), f32),
            jax.ShapeDtypeStruct((heads, tok, 2 * n), bf16),
            jax.ShapeDtypeStruct((heads, 2 * NBLK, n, 2 * n), bf16),
            jax.ShapeDtypeStruct((heads, 2, n, 2 * n), bf16),
        ],
        compiler_params=ARB,
        name="local_pass",
    )(queries, keys, values, log_decay, beta)


def exchange_kernel(comp_ref, out_ref, got, pre, chunk, start, ready, send1, recv1, send2, recv2):
    n = BLOCK
    z, y, core = (lax.axis_index(a) for a in SP)
    me = (z * 4 + y) * 2 + core
    is_owner = jnp.logical_and(core == 1, y % 2 == z % 2)
    way = y // 2
    mine = z * 2 + way

    def place(s):
        return {"sp_0": s // 8, "sp_1": (s // 2) % 4, "sp_2": s % 2}

    barrier = pltpu.get_barrier_semaphore()

    def greet(i, carry):
        other = (me + i) % 32
        pl.semaphore_signal(barrier, inc=1, device_id=place(other), device_id_type=MESH)
        return carry

    lax.fori_loop(1, 32, greet, 0)
    pl.semaphore_wait(barrier, 31)

    def owner_of(c):
        oz = c // 2
        return (oz * 4 + (c % 2) * 2 + oz % 2) * 2 + 1

    def first_copy(c):
        return pltpu.make_async_remote_copy(
            src_ref=comp_ref.at[c],
            dst_ref=got.at[me],
            send_sem=send1.at[c],
            recv_sem=recv1.at[me],
            device_id=place(owner_of(c)),
            device_id_type=MESH,
        )

    for c in range(8):
        own = owner_of(c)

        @pl.when(me != own)
        def _():
            first_copy(c).start()

        @pl.when(me == own)
        def _():
            got[me] = comp_ref[c]

    def arrival(s):
        return pltpu.make_async_remote_copy(
            src_ref=comp_ref.at[0],
            dst_ref=got.at[s],
            send_sem=send1.at[0],
            recv_sem=recv1.at[s],
            device_id=place(s),
            device_id_type=MESH,
        )

    def second_copy(p, s):
        return pltpu.make_async_remote_copy(
            src_ref=ready.at[p],
            dst_ref=out_ref.at[mine],
            send_sem=send2.at[p],
            recv_sem=recv2.at[mine],
            device_id=place(s),
            device_id_type=MESH,
        )

    @pl.when(is_owner)
    def _():
        row = lax.broadcasted_iota(jnp.int32, (n, 2 * n), 0)
        col = lax.broadcasted_iota(jnp.int32, (n, 2 * n), 1)
        unit = (row + n == col).astype(f32)
        for j in range(4):
            chunk[j] = unit

        def step(r, carry):
            for j in range(4):
                p = 8 * j + r
                s = p + way * (31 - 2 * p)

                @pl.when(s != me)
                def _():
                    arrival(s).wait_recv()

                now = chunk[j].astype(bf16)
                pre[p] = now
                moved = mm(got[s, :, n:], now)
                chunk[j, :, :n] = moved[:, :n] + got[s, :, :n].astype(f32)
                chunk[j, :, n:] = moved[:, n:]
            return carry

        lax.fori_loop(0, 8, step, 0)
        start[0] = jnp.zeros((n, n), bf16)
        held = jnp.zeros((n, n), f32)
        for j in range(3):
            held = mm(chunk[j, :, n:].astype(bf16), held.astype(bf16)) + chunk[j, :, :n]
            start[j + 1] = held.astype(bf16)

        def finish(r, carry):
            for j in range(4):
                p = 8 * j + r
                s = p + way * (31 - 2 * p)
                given = mm(pre[p, :, n:], start[j]) + pre[p, :, :n].astype(f32)
                ready[p] = given.astype(bf16)

                @pl.when(s != me)
                def _():
                    second_copy(p, s).start()

                @pl.when(s == me)
                def _():
                    out_ref[mine] = given.astype(bf16)

            return carry

        lax.fori_loop(0, 8, finish, 0)

        def drain(p, carry):
            s = p + way * (31 - 2 * p)

            @pl.when(s != me)
            def _():
                second_copy(p, s).wait_send()

            return carry

        lax.fori_loop(0, 32, drain, 0)

    for c in range(8):

        @pl.when(me != owner_of(c))
        def _():
            first_copy(c).wait_send()
            pltpu.make_async_remote_copy(
                src_ref=ready.at[0],
                dst_ref=out_ref.at[c],
                send_sem=send2.at[0],
                recv_sem=recv2.at[c],
                device_id=place(owner_of(c)),
                device_id_type=MESH,
            ).wait_recv()


def exchange(comp):
    n = BLOCK
    return pl.pallas_call(
        exchange_kernel,
        in_specs=[pl.BlockSpec(memory_space=pltpu.VMEM)],
        out_specs=pl.BlockSpec(memory_space=pltpu.VMEM),
        out_shape=jax.ShapeDtypeStruct((8, n, n), bf16),
        scratch_shapes=[
            pltpu.VMEM((32, n, 2 * n), bf16),
            pltpu.VMEM((32, n, 2 * n), bf16),
            pltpu.VMEM((4, n, 2 * n), f32),
            pltpu.VMEM((4, n, n), bf16),
            pltpu.VMEM((32, n, n), bf16),
            pltpu.SemaphoreType.DMA((8,)),
            pltpu.SemaphoreType.DMA((32,)),
            pltpu.SemaphoreType.DMA((32,)),
            pltpu.SemaphoreType.DMA((8,)),
        ],
        compiler_params=pltpu.CompilerParams(collective_id=0, has_side_effects=True),
        name="exchange",
    )(comp)


def finish_kernel(out_ref, qeff_ref, blk_ref, sin_ref, gate_ref, gain_ref, mix_ref):
    n = BLOCK
    gain = gain_ref[...].astype(f32)
    states = {}
    held = [sin_ref[0, d].astype(f32) for d in range(2)]
    for step in range(NBLK):
        for d in range(2):
            b = step if d == 0 else NBLK - 1 - step
            states[d, b] = held[d].astype(bf16)
            if step < NBLK - 1:
                i = d * NBLK + b
                held[d] = mm(blk_ref[0, i, :, n:], states[d, b]) + blk_ref[0, i, :, :n].astype(f32)
    for b in range(NBLK):
        rows = pl.ds(b * n, n)
        both = jnp.concatenate([states[0, b], states[1, b]], axis=0)
        o = out_ref[rows, :] + mm(qeff_ref[0, rows, :], both)
        o = o * lax.rsqrt(jnp.mean(o * o, axis=-1, keepdims=True) + 1e-06) * gain
        g = gate_ref[rows, :].astype(f32)
        mix_ref[rows, :] = (o * (g * jax.nn.sigmoid(g))).astype(bf16)


def finish_pass(out_local, qeff, blk, entering, gates, gain):
    tok, width = out_local.shape
    n = BLOCK
    heads = width // n
    columns = pl.BlockSpec((tok, n), lambda h: (0, h))
    return pl.pallas_call(
        finish_kernel,
        grid=(heads,),
        in_specs=[
            columns,
            pl.BlockSpec((1, tok, 2 * n), lambda h: (h, 0, 0)),
            pl.BlockSpec((1, 2 * NBLK, n, 2 * n), lambda h: (h, 0, 0, 0)),
            pl.BlockSpec((1, 2, n, n), lambda h: (h, 0, 0, 0)),
            columns,
            pl.BlockSpec((1, n), lambda h: (0, 0)),
        ],
        out_specs=columns,
        out_shape=jax.ShapeDtypeStruct((tok, width), bf16),
        compiler_params=ARB,
        name="finish_pass",
    )(out_local, qeff, blk, entering, gates, gain)


def head_mixing(queries, keys, values, gates, decay_logits, write_logits, extra, rate, gain):
    tok, width = queries.shape
    heads = width // HEAD_DIM
    log_decay = -rate[:, None, :] * jax.nn.softplus(decay_logits) + extra
    beta = jax.nn.sigmoid(write_logits)

    def per_head(t):
        t = t.transpose(2, 0, 1).reshape(heads, 2 * NBLK, BLOCK)
        return t

    out_local, qeff, blk, comp = local_pass(
        queries, keys, values, per_head(log_decay), per_head(beta), heads
    )
    entering = exchange(comp.reshape(2 * heads, BLOCK, 2 * BLOCK))
    return finish_pass(
        out_local, qeff, blk, entering.reshape(heads, 2, BLOCK, BLOCK), gates, gain.reshape(1, -1)
    )


def in_blocks(shard, dim, count):
    shape = shard.shape
    parts = shard.reshape(*shape[:dim], count, shape[dim] // count, *shape[dim + 1 :])
    return jnp.moveaxis(parts, dim, 0)


def summed_on_arrival(shard, axis, dim):
    parts = in_blocks(shard, dim, lax.axis_size(axis))
    arrived = lax.all_to_all(parts, axis, split_axis=0, concat_axis=0, tiled=True)
    return arrived.astype(jnp.float32).sum(axis=0)


def per_device(
    queries,
    keys,
    values,
    output_gate_logits,
    decay_gate_logits,
    write_strength_logits,
    extra_log_decay,
    head_decay_rate,
    head_norm_gain,
    output_weight,
    residual,
    expert_norm_gain,
    selected_experts,
    router_chosen_scores,
    gate_up_weight,
    linear_up_weight,
    down_weight,
):
    tok_rows, width_dev = queries.shape
    head_mix = head_mixing(
        queries,
        keys,
        values,
        output_gate_logits,
        decay_gate_logits,
        write_strength_logits,
        extra_log_decay,
        head_decay_rate,
        head_norm_gain,
    )
    local_rows = residual.shape[0]
    mix_sum = summed_on_arrival(
        jnp.dot(head_mix, output_weight, preferred_element_type=jnp.float32).astype(jnp.bfloat16),
        "tp",
        0,
    )
    stream = (residual.astype(jnp.float32) + mix_sum).astype(jnp.bfloat16)
    stream_wide = stream.astype(jnp.float32)
    normed = (
        stream_wide
        * lax.rsqrt(jnp.mean(stream_wide * stream_wide, axis=-1, keepdims=True) + 1e-06)
        * expert_norm_gain.astype(jnp.float32)
    ).astype(jnp.bfloat16)
    route_exp = jnp.exp(router_chosen_scores)
    route_weight = route_exp / jnp.sum(route_exp, axis=-1, keepdims=True)
    sp_count = lax.axis_size(SP)
    tp_count = lax.axis_size("tp")
    exp_dev = gate_up_weight.shape[0]
    experts = exp_dev * sp_count
    capacity = 3 * TOPK * tok_rows // (2 * tp_count * experts)
    model_width = normed.shape[1]
    flat_experts = selected_experts.reshape(-1)
    member = (flat_experts[:, None] == jnp.arange(experts, dtype=jnp.int32)[None, :]).astype(
        jnp.int32
    )
    slot_rank = jnp.sum(jnp.cumsum(member, axis=0) * member, axis=1) - 1
    slot_index = flat_experts * capacity + slot_rank
    slot_hot = (
        slot_index[:, None] == jnp.arange(experts * capacity, dtype=jnp.int32)[None, :]
    ).astype(jnp.bfloat16)
    token_hot = jnp.sum(slot_hot.reshape(local_rows, TOPK, experts * capacity), axis=1)
    outgoing = jnp.einsum(
        "rs,rd->sd", token_hot, normed, preferred_element_type=jnp.float32
    ).astype(jnp.bfloat16)
    grouped = outgoing.reshape(sp_count, exp_dev, capacity, model_width)
    copies = jnp.broadcast_to(
        grouped[:, None], (sp_count, tp_count, exp_dev, capacity, model_width)
    )
    copies = copies.reshape(sp_count * tp_count, exp_dev, capacity, model_width)
    arrived = lax.all_to_all(copies, SP_TP, split_axis=0, concat_axis=0, tiled=True)
    gate_pre = jnp.einsum(
        "secd,edf->secf", arrived, gate_up_weight, preferred_element_type=jnp.float32
    )
    linear_pre = jnp.einsum(
        "secd,edf->secf", arrived, linear_up_weight, preferred_element_type=jnp.float32
    )
    clipped = jnp.minimum(gate_pre, 7.0)
    hidden_act = (
        clipped * jax.nn.sigmoid(1.702 * clipped) * (jnp.clip(linear_pre, -7.0, 7.0) + 1.0)
    ).astype(jnp.bfloat16)
    partial_value = jnp.einsum(
        "secf,efd->secd", hidden_act, down_weight, preferred_element_type=jnp.float32
    )
    summed = lax.psum_scatter(
        partial_value.reshape(sp_count, tp_count, exp_dev, capacity, model_width).astype(
            jnp.bfloat16
        ),
        "tp",
        scatter_dimension=1,
        tiled=True,
    )
    returned = lax.all_to_all(summed, SP, split_axis=0, concat_axis=0, tiled=True)
    returned = returned.reshape(experts * capacity, model_width)
    picked = jnp.dot(slot_hot, returned, preferred_element_type=jnp.float32).reshape(
        local_rows, TOPK, model_width
    )
    combined = jnp.sum(picked * route_weight[:, :, None], axis=1)
    return (stream_wide + combined).astype(jnp.bfloat16)


def solution(mesh):
    torus = Mesh(mesh.devices.reshape(4, 4, 2, mesh.shape["tp"]), ("sp_0", "sp_1", "sp_2", "tp"))
    placed = (
        P(SP, "tp"),
        P(SP, "tp"),
        P(SP, "tp"),
        P(SP, "tp"),
        P(None, SP, "tp"),
        P(None, SP, "tp"),
        P(None, SP, "tp"),
        P(None, "tp"),
        P(),
        P("tp", None),
        P(SP_TP, None),
        P(),
        P(SP_TP, None),
        P(SP_TP, None),
        P(SP, None, "tp"),
        P(SP, None, "tp"),
        P(SP, "tp", None),
    )
    return jax.shard_map(
        per_device, mesh=torus, in_specs=placed, out_specs=P(SP_TP, None), check_vma=False
    )
```

```python
import jax
import jax.numpy as jnp
from jax import lax
from jax.experimental import pallas as pl
from jax.experimental.pallas import tpu as pltpu
from jax.sharding import Mesh
from jax.sharding import PartitionSpec as P

HEAD_DIM = 128
TOPK = 2
BLOCK = 128
SP = ("sp_0", "sp_1", "sp_2")
SP_TP = ("sp_0", "sp_1", "sp_2", "tp")
ARB = pltpu.CompilerParams(dimension_semantics=("arbitrary",), vmem_limit_bytes=48 * 1024 * 1024)
MESH = pl.DeviceIdType.MESH
NBLK = 4
f32 = jnp.float32
bf16 = jnp.bfloat16


def mm(a, b):
    return jnp.dot(a, b, preferred_element_type=f32)


def local_kernel(q_ref, k_ref, v_ref, ld_ref, bt_ref, out_ref, qeff_ref, blk_ref, comp_ref):
    n = BLOCK
    row = lax.broadcasted_iota(jnp.int32, (n, n), 0)
    col = lax.broadcasted_iota(jnp.int32, (n, n), 1)
    upper = (row <= col).astype(f32)
    lower = (row >= col).astype(f32)
    eye = (row == col).astype(f32)
    ld = ld_ref[0]
    highest = lax.Precision.HIGHEST
    run_f = jnp.dot(ld, upper, precision=highest, preferred_element_type=f32)
    run_b = jnp.dot(ld, lower, precision=highest, preferred_element_type=f32)
    which = lax.broadcasted_iota(jnp.int32, (2 * NBLK, n), 0)
    cum_rows = jnp.where(which < NBLK, run_f, run_b)
    cum_cols = jnp.transpose(cum_rows)
    beta_cols = jnp.transpose(bt_ref[0])
    chains = [(d, b) for d in range(2) for b in range(NBLK)]
    grams, k_un, v_un, q_un, kt_un = [], [], [], [], []
    for b in range(NBLK):
        rows = pl.ds(b * n, n)
        q = q_ref[rows, :].astype(f32)
        k = k_ref[rows, :].astype(f32)
        q = q * lax.rsqrt(jnp.sum(q * q, axis=-1, keepdims=True) + 1e-06) * HEAD_DIM ** (-0.5)
        k = k * lax.rsqrt(jnp.sum(k * k, axis=-1, keepdims=True) + 1e-06)
        kt = jnp.transpose(k).astype(bf16)
        grams.append((mm(k.astype(bf16), kt), mm(q.astype(bf16), kt)))
        q_un.append(q)
        k_un.append(k)
        kt_un.append(kt)
        v_un.append(v_ref[rows, :].astype(f32))
    low, attn, sums, pows = {}, {}, {}, {}
    for d, b in chains:
        i = d * NBLK + b
        gap = cum_cols[:, i : i + 1] - cum_rows[i : i + 1, :]
        keep = row >= col if d == 0 else row <= col
        decay = jnp.exp(jnp.where(keep, gap, -1e30))
        attn[d, b] = (grams[b][1] * decay).astype(bf16)
        strict = row > col if d == 0 else row < col
        low = jnp.where(strict, grams[b][0] * decay, 0.0) * beta_cols[:, i : i + 1]
        sums[d, b] = eye - low
        pows[d, b] = low.astype(bf16)
    for c in chains:
        pows[c] = mm(pows[c], pows[c]).astype(bf16)
    for step in range(5):
        for c in chains:
            both = mm(jnp.concatenate([sums[c].astype(bf16), pows[c]], axis=0), pows[c])
            sums[c] = sums[c] + both[:n]
            pows[c] = both[n:].astype(bf16)
    for c in chains:
        sums[c] = sums[c] + mm(sums[c].astype(bf16), pows[c])
    fresh, maps = {}, {}
    for d, b in chains:
        i = d * NBLK + b
        cc = cum_cols[:, i : i + 1]
        bt = beta_cols[:, i : i + 1]
        right = jnp.concatenate([v_un[b] * bt, k_un[b] * (-bt * jnp.exp(cc))], axis=1)
        fresh[d, b] = mm(sums[d, b].astype(bf16), right.astype(bf16))
    for d, b in chains:
        i = d * NBLK + b
        cc = cum_cols[:, i : i + 1]
        last = n - 1 if d == 0 else 0
        total = cum_rows[i : i + 1, last : last + 1]
        ended = (fresh[d, b] * jnp.exp(total - cc)).astype(bf16)
        step_map = mm(kt_un[b], ended) + jnp.concatenate(
            [jnp.zeros((n, n), f32), eye * jnp.exp(total)], axis=1
        )
        maps[d, b] = step_map
        blk_ref[0, i] = step_map.astype(bf16)
    for b in range(NBLK):
        rows = pl.ds(b * n, n)
        locals_, effs = [], []
        for d in range(2):
            i = d * NBLK + b
            given = mm(attn[d, b], fresh[d, b].astype(bf16))
            locals_.append(given[:, :n])
            effs.append(given[:, n:] + q_un[b] * jnp.exp(cum_cols[:, i : i + 1]))
        out_ref[rows, :] = locals_[0] + locals_[1]
        qeff_ref[0, rows, :] = jnp.concatenate(effs, axis=1).astype(bf16)

    def after(later, earlier):
        moved = mm(later[:, n:].astype(bf16), earlier.astype(bf16))
        return jnp.concatenate([moved[:, :n] + later[:, :n], moved[:, n:]], axis=1)

    for d in range(2):
        order = range(NBLK) if d == 0 else range(NBLK - 1, -1, -1)
        first, second, third, fourth = [maps[d, b] for b in order]
        comp_ref[0, d] = after(after(fourth, third), after(second, first)).astype(bf16)


def local_pass(queries, keys, values, log_decay, beta, heads):
    tok = queries.shape[0]
    n = BLOCK
    columns = pl.BlockSpec((tok, n), lambda h: (0, h))
    small = pl.BlockSpec((1, 2 * NBLK, n), lambda h: (h, 0, 0))
    return pl.pallas_call(
        local_kernel,
        grid=(heads,),
        in_specs=[columns, columns, columns, small, small],
        out_specs=[
            columns,
            pl.BlockSpec((1, tok, 2 * n), lambda h: (h, 0, 0)),
            pl.BlockSpec((1, 2 * NBLK, n, 2 * n), lambda h: (h, 0, 0, 0)),
            pl.BlockSpec((1, 2, n, 2 * n), lambda h: (h, 0, 0, 0)),
        ],
        out_shape=[
            jax.ShapeDtypeStruct((tok, heads * n), f32),
            jax.ShapeDtypeStruct((heads, tok, 2 * n), bf16),
            jax.ShapeDtypeStruct((heads, 2 * NBLK, n, 2 * n), bf16),
            jax.ShapeDtypeStruct((heads, 2, n, 2 * n), bf16),
        ],
        compiler_params=ARB,
        name="local_pass",
    )(queries, keys, values, log_decay, beta)


def exchange_kernel(comp_ref, out_ref, got, pre, chunk, start, ready, send1, recv1, send2, recv2):
    n = BLOCK
    z, y, core = (lax.axis_index(a) for a in SP)
    me = (z * 4 + y) * 2 + core
    is_owner = jnp.logical_and(core == 1, y % 2 == z % 2)
    way = y // 2
    mine = z * 2 + way

    def place(s):
        return {"sp_0": s // 8, "sp_1": (s // 2) % 4, "sp_2": s % 2}

    barrier = pltpu.get_barrier_semaphore()

    def greet(i, carry):
        other = (me + i) % 32
        pl.semaphore_signal(barrier, inc=1, device_id=place(other), device_id_type=MESH)
        return carry

    lax.fori_loop(1, 32, greet, 0)
    pl.semaphore_wait(barrier, 31)

    def owner_of(c):
        oz = c // 2
        return (oz * 4 + (c % 2) * 2 + oz % 2) * 2 + 1

    def first_copy(c):
        return pltpu.make_async_remote_copy(
            src_ref=comp_ref.at[c],
            dst_ref=got.at[me],
            send_sem=send1.at[c],
            recv_sem=recv1.at[me],
            device_id=place(owner_of(c)),
            device_id_type=MESH,
        )

    for c in range(8):
        own = owner_of(c)

        @pl.when(me != own)
        def _():
            first_copy(c).start()

        @pl.when(me == own)
        def _():
            got[me] = comp_ref[c]

    def arrival(s):
        return pltpu.make_async_remote_copy(
            src_ref=comp_ref.at[0],
            dst_ref=got.at[s],
            send_sem=send1.at[0],
            recv_sem=recv1.at[s],
            device_id=place(s),
            device_id_type=MESH,
        )

    def second_copy(p, s):
        return pltpu.make_async_remote_copy(
            src_ref=ready.at[p],
            dst_ref=out_ref.at[mine],
            send_sem=send2.at[p],
            recv_sem=recv2.at[mine],
            device_id=place(s),
            device_id_type=MESH,
        )

    @pl.when(is_owner)
    def _():
        row = lax.broadcasted_iota(jnp.int32, (n, 2 * n), 0)
        col = lax.broadcasted_iota(jnp.int32, (n, 2 * n), 1)
        unit = (row + n == col).astype(f32)
        for j in range(4):
            chunk[j] = unit

        def step(r, carry):
            for j in range(4):
                p = 8 * j + r
                s = p + way * (31 - 2 * p)

                @pl.when(s != me)
                def _():
                    arrival(s).wait_recv()

                now = chunk[j].astype(bf16)
                pre[p] = now
                moved = mm(got[s, :, n:], now)
                chunk[j, :, :n] = moved[:, :n] + got[s, :, :n].astype(f32)
                chunk[j, :, n:] = moved[:, n:]
            return carry

        lax.fori_loop(0, 8, step, 0)
        start[0] = jnp.zeros((n, n), bf16)
        held = jnp.zeros((n, n), f32)
        for j in range(3):
            held = mm(chunk[j, :, n:].astype(bf16), held.astype(bf16)) + chunk[j, :, :n]
            start[j + 1] = held.astype(bf16)

        def finish(r, carry):
            for j in range(4):
                p = 8 * j + r
                s = p + way * (31 - 2 * p)
                given = mm(pre[p, :, n:], start[j]) + pre[p, :, :n].astype(f32)
                ready[p] = given.astype(bf16)

                @pl.when(s != me)
                def _():
                    second_copy(p, s).start()

                @pl.when(s == me)
                def _():
                    out_ref[mine] = given.astype(bf16)

            return carry

        lax.fori_loop(0, 8, finish, 0)

        def drain(p, carry):
            s = p + way * (31 - 2 * p)

            @pl.when(s != me)
            def _():
                second_copy(p, s).wait_send()

            return carry

        lax.fori_loop(0, 32, drain, 0)

    for c in range(8):

        @pl.when(me != owner_of(c))
        def _():
            first_copy(c).wait_send()
            pltpu.make_async_remote_copy(
                src_ref=ready.at[0],
                dst_ref=out_ref.at[c],
                send_sem=send2.at[0],
                recv_sem=recv2.at[c],
                device_id=place(owner_of(c)),
                device_id_type=MESH,
            ).wait_recv()


def exchange(comp):
    n = BLOCK
    return pl.pallas_call(
        exchange_kernel,
        in_specs=[pl.BlockSpec(memory_space=pltpu.VMEM)],
        out_specs=pl.BlockSpec(memory_space=pltpu.VMEM),
        out_shape=jax.ShapeDtypeStruct((8, n, n), bf16),
        scratch_shapes=[
            pltpu.VMEM((32, n, 2 * n), bf16),
            pltpu.VMEM((32, n, 2 * n), bf16),
            pltpu.VMEM((4, n, 2 * n), f32),
            pltpu.VMEM((4, n, n), bf16),
            pltpu.VMEM((32, n, n), bf16),
            pltpu.SemaphoreType.DMA((8,)),
            pltpu.SemaphoreType.DMA((32,)),
            pltpu.SemaphoreType.DMA((32,)),
            pltpu.SemaphoreType.DMA((8,)),
        ],
        compiler_params=pltpu.CompilerParams(collective_id=0, has_side_effects=True),
        name="exchange",
    )(comp)


def finish_kernel(out_ref, qeff_ref, blk_ref, sin_ref, gate_ref, gain_ref, mix_ref):
    n = BLOCK
    gain = gain_ref[...].astype(f32)
    states = {}
    held = [sin_ref[0, d].astype(f32) for d in range(2)]
    for step in range(NBLK):
        for d in range(2):
            b = step if d == 0 else NBLK - 1 - step
            states[d, b] = held[d].astype(bf16)
            if step < NBLK - 1:
                i = d * NBLK + b
                held[d] = mm(blk_ref[0, i, :, n:], states[d, b]) + blk_ref[0, i, :, :n].astype(f32)
    for b in range(NBLK):
        rows = pl.ds(b * n, n)
        both = jnp.concatenate([states[0, b], states[1, b]], axis=0)
        o = out_ref[rows, :] + mm(qeff_ref[0, rows, :], both)
        o = o * lax.rsqrt(jnp.mean(o * o, axis=-1, keepdims=True) + 1e-06) * gain
        g = gate_ref[rows, :].astype(f32)
        mix_ref[rows, :] = (o * (g * jax.nn.sigmoid(g))).astype(bf16)


def finish_pass(out_local, qeff, blk, entering, gates, gain):
    tok, width = out_local.shape
    n = BLOCK
    heads = width // n
    columns = pl.BlockSpec((tok, n), lambda h: (0, h))
    return pl.pallas_call(
        finish_kernel,
        grid=(heads,),
        in_specs=[
            columns,
            pl.BlockSpec((1, tok, 2 * n), lambda h: (h, 0, 0)),
            pl.BlockSpec((1, 2 * NBLK, n, 2 * n), lambda h: (h, 0, 0, 0)),
            pl.BlockSpec((1, 2, n, n), lambda h: (h, 0, 0, 0)),
            columns,
            pl.BlockSpec((1, n), lambda h: (0, 0)),
        ],
        out_specs=columns,
        out_shape=jax.ShapeDtypeStruct((tok, width), bf16),
        compiler_params=ARB,
        name="finish_pass",
    )(out_local, qeff, blk, entering, gates, gain)


def head_mixing(queries, keys, values, gates, decay_logits, write_logits, extra, rate, gain):
    tok, width = queries.shape
    heads = width // HEAD_DIM
    log_decay = -rate[:, None, :] * jax.nn.softplus(decay_logits) + extra
    beta = jax.nn.sigmoid(write_logits)

    def per_head(t):
        t = t.transpose(2, 0, 1).reshape(heads, 2 * NBLK, BLOCK)
        return t

    out_local, qeff, blk, comp = local_pass(
        queries, keys, values, per_head(log_decay), per_head(beta), heads
    )
    entering = exchange(comp.reshape(2 * heads, BLOCK, 2 * BLOCK))
    return finish_pass(
        out_local, qeff, blk, entering.reshape(heads, 2, BLOCK, BLOCK), gates, gain.reshape(1, -1)
    )


def in_blocks(shard, dim, count):
    shape = shard.shape
    parts = shard.reshape(*shape[:dim], count, shape[dim] // count, *shape[dim + 1 :])
    return jnp.moveaxis(parts, dim, 0)


def summed_on_arrival(shard, axis, dim):
    parts = in_blocks(shard, dim, lax.axis_size(axis))
    arrived = lax.all_to_all(parts, axis, split_axis=0, concat_axis=0, tiled=True)
    return arrived.astype(jnp.float32).sum(axis=0)


PLANE = (
    (0, 0), (0, 1), (1, 0), (0, 3), (3, 0), (1, 1), (3, 3), (1, 3),
    (3, 1), (0, 2), (2, 0), (1, 2), (3, 2), (2, 1), (2, 3), (2, 2),
)
ORDER = tuple((dz, dy, dc) for dz, dy in PLANE for dc in range(2))
CAP = 12
SLOTS = len(ORDER)
HALF = 2048
FFD = 384
ROWS = SLOTS * CAP


def plane_place(z, y, core, offset, sign):
    dz, dy, dc = offset
    return {
        "sp_0": lax.rem(z + (dz if sign > 0 else 4 - dz), 4),
        "sp_1": lax.rem(y + (dy if sign > 0 else 4 - dy), 4),
        "sp_2": lax.rem(core + dc, 2),
    }


def greet_all(z, y, core, x, around):
    barrier = pltpu.get_barrier_semaphore()
    for offset in ORDER[1:]:
        pl.semaphore_signal(
            barrier, inc=1, device_id=plane_place(z, y, core, offset, 1), device_id_type=MESH
        )
    count = SLOTS - 1
    if around:
        for dx in range(1, 4):
            pl.semaphore_signal(
                barrier, inc=1, device_id={"tp": lax.rem(x + dx, 4)}, device_id_type=MESH
            )
        count += 3
    pl.semaphore_wait(barrier, count)


def dispatch_kernel(
    blocks_ref, gate_ref, lin_ref, hid_ref,
    xb, wg, wl, rows_buf, act_buf,
    wsem, send0, send1, send2, send3, recv, hsend, hrecv,
):
    z, y, core = (lax.axis_index(a) for a in SP)
    x = lax.axis_index("tp")
    right, left, far = lax.rem(x + 1, 4), lax.rem(x + 3, 4), lax.rem(x + 2, 4)
    load_g = pltpu.make_async_copy(gate_ref, wg, wsem.at[0])
    load_l = pltpu.make_async_copy(lin_ref, wl, wsem.at[1])
    load_g.start()
    load_l.start()
    greet_all(z, y, core, x, True)

    def plane_copy(i):
        return pltpu.make_async_remote_copy(
            src_ref=blocks_ref.at[i], dst_ref=xb.at[0, i], send_sem=send0.at[i],
            recv_sem=recv.at[0, i], device_id=plane_place(z, y, core, ORDER[i], 1),
            device_id_type=MESH,
        )

    def line_copy(src, group, i, sem, to):
        return pltpu.make_async_remote_copy(
            src_ref=src, dst_ref=xb.at[group, i], send_sem=sem.at[i],
            recv_sem=recv.at[group, i], device_id={"tp": to}, device_id_type=MESH,
        )

    def own(i):
        return blocks_ref.at[i] if i == 0 else xb.at[0, i]

    for i in range(1, SLOTS):
        plane_copy(i).start()
    xb[0, 0] = blocks_ref[0]
    for i in range(SLOTS):
        if i:
            plane_copy(i).wait_recv()
        line_copy(own(i), 1, i, send1, right).start()
        line_copy(own(i), 2, i, send2, left).start()
    load_g.wait()
    load_l.wait()
    r = lax.broadcasted_iota(jnp.int32, (192, 192), 0)
    c = lax.broadcasted_iota(jnp.int32, (192, 192), 1)
    within = lax.rem(r, 96)
    source = (within // CAP) * (2 * CAP) + (r // 96) * CAP + lax.rem(within, CAP)
    perm = (c == source).astype(f32).astype(bf16)

    def compute(group, part):
        for s in range(2):
            for q in range(4):
                cols = pl.ds(q * 512, 512)
                raw = xb[group, pl.ds(part * 16 + s * 8, 8), :, cols].reshape(192, 512)
                fixed = mm(perm, raw).astype(bf16)
                rows_buf[pl.ds(s * 96, 96), cols] = fixed[:96]
                rows_buf[pl.ds(s * 96, 96), pl.ds(HALF + q * 512, 512)] = fixed[96:]
        gate = mm(rows_buf[...], wg[...])
        lin = mm(rows_buf[...], wl[...])
        gate = jnp.minimum(gate, 7.0)
        act = gate * jax.nn.sigmoid(1.702 * gate) * (jnp.clip(lin, -7.0, 7.0) + 1.0)
        act_buf[group, pl.ds(part * 192, 192), :] = act.astype(bf16)

    def hid_copy(group, to):
        return pltpu.make_async_remote_copy(
            src_ref=act_buf.at[group], dst_ref=hid_ref.at[x], send_sem=hsend.at[group],
            recv_sem=hrecv.at[x], device_id={"tp": to}, device_id_type=MESH,
        )

    def relay(part):
        def one(j, carry):
            a = part * 16 + 2 * j
            b = a + 1
            line_copy(xb.at[0, 0], 1, a, send1, right).wait_recv()
            line_copy(xb.at[1, a], 3, a, send3, right).start()
            line_copy(xb.at[0, 0], 2, b, send2, left).wait_recv()
            line_copy(xb.at[2, b], 3, b, send3, left).start()
            line_copy(xb.at[0, 0], 1, b, send1, right).wait_recv()
            line_copy(xb.at[0, 0], 2, a, send2, left).wait_recv()
            return carry

        lax.fori_loop(0, 8, one, 0)

    def far_wait(part):
        def one(j, carry):
            line_copy(xb.at[0, 0], 3, part * 16 + j, send3, far).wait_recv()
            return carry

        lax.fori_loop(0, 16, one, 0)

    def turn(t, carry):
        @pl.when(jnp.logical_or(t == 2, t == 4))
        def _():
            relay((t - 2) // 2)

        @pl.when(t >= 6)
        def _():
            far_wait(t - 6)

        middle = jnp.logical_and(t >= 2, t < 6)
        group = jnp.where(t < 2, 0, jnp.where(middle, 1 + lax.rem(t, 2), 3))
        part = jnp.where(t < 2, t, jnp.where(middle, (t - 2) // 2, t - 6))
        compute(group, part)

        @pl.when(t == 4)
        def _():
            hid_copy(1, left).start()

        @pl.when(t == 5)
        def _():
            hid_copy(2, right).start()

        return carry

    lax.fori_loop(0, 8, turn, 0)
    hid_copy(3, far).start()
    hid_ref[x] = act_buf[0]
    for group, to in ((1, left), (2, right), (3, far)):
        hid_copy(group, to).wait_send()
        pltpu.make_async_remote_copy(
            src_ref=act_buf.at[group], dst_ref=hid_ref.at[to], send_sem=hsend.at[group],
            recv_sem=hrecv.at[to], device_id={"tp": to}, device_id_type=MESH,
        ).wait_recv()
    for i in range(SLOTS):
        if i:
            plane_copy(i).wait_send()
        line_copy(own(i), 1, i, send1, right).wait_send()
        line_copy(own(i), 2, i, send2, left).wait_send()
        line_copy(xb.at[1, i], 3, i, send3, right).wait_send()


def dispatch(blocks, gate_w, lin_w):
    width = gate_w.shape[0]
    dma = pltpu.SemaphoreType.DMA
    return pl.pallas_call(
        dispatch_kernel,
        in_specs=[
            pl.BlockSpec(memory_space=pltpu.VMEM),
            pl.BlockSpec(memory_space=pl.ANY),
            pl.BlockSpec(memory_space=pl.ANY),
        ],
        out_specs=pl.BlockSpec(memory_space=pltpu.VMEM),
        out_shape=jax.ShapeDtypeStruct((4, ROWS, FFD), bf16),
        scratch_shapes=[
            pltpu.VMEM((4, SLOTS, 2 * CAP, HALF), bf16),
            pltpu.VMEM((width, FFD), bf16),
            pltpu.VMEM((width, FFD), bf16),
            pltpu.VMEM((192, width), bf16),
            pltpu.VMEM((4, ROWS, FFD), bf16),
            dma((2,)), dma((SLOTS,)), dma((SLOTS,)), dma((SLOTS,)), dma((SLOTS,)),
            dma((4, SLOTS)), dma((4,)), dma((4,)),
        ],
        compiler_params=pltpu.CompilerParams(
            collective_id=1, has_side_effects=True, vmem_limit_bytes=56 * 1024 * 1024
        ),
        name="dispatch",
    )(blocks, gate_w, lin_w)


TILE = 512


def return_kernel(
    hid_ref, down_ref, index_ref, weight_ref, stream_ref, out_ref,
    wd, ready, back, pair_buf, wsem, sends, recvs,
):
    z, y, core = (lax.axis_index(a) for a in SP)
    x = lax.axis_index("tp")
    steps = HALF // TILE

    def load(j, h):
        cols = pl.ds(h * HALF + j * TILE, TILE)
        return pltpu.make_async_copy(down_ref.at[:, cols], wd.at[j, h], wsem.at[j, h])

    for j in range(steps):
        for h in range(2):
            load(j, h).start()
    greet_all(z, y, core, x, False)
    r = lax.broadcasted_iota(jnp.int32, (192, 192), 0)
    c = lax.broadcasted_iota(jnp.int32, (192, 192), 1)
    within = lax.rem(r, 2 * CAP)
    source = (within // CAP) * 96 + (r // (2 * CAP)) * CAP + lax.rem(within, CAP)
    perm = (c == source).astype(f32).astype(bf16)

    def send(i, j):
        return pltpu.make_async_remote_copy(
            src_ref=ready.at[j, i], dst_ref=back.at[j, i], send_sem=sends.at[j, i],
            recv_sem=recvs.at[j, i], device_id=plane_place(z, y, core, ORDER[i], -1),
            device_id_type=MESH,
        )

    for j in range(steps):
        for h in range(2):
            load(j, h).wait()
            total = mm(hid_ref[0], wd[j, h, pl.ds(0, FFD), :])
            for k in range(1, 4):
                total = total + mm(hid_ref[k], wd[j, h, pl.ds(k * FFD, FFD), :])
            pair_buf[h] = total.astype(bf16)
        for q in range(4):
            rows = pl.ds(q * 96, 96)
            both = jnp.concatenate([pair_buf[0, rows, :], pair_buf[1, rows, :]], axis=0)
            mixed = mm(perm, both).astype(bf16).reshape(8, 2 * CAP, TILE)
            ready[j, pl.ds(q * 8, 8)] = mixed
            for i in range(q * 8, q * 8 + 8):
                if i:
                    send(i, j).start()
        back[j, 0] = ready[j, 0]
    slots = lax.broadcasted_iota(jnp.int32, (512, SLOTS * 2 * CAP), 1)
    hot = (slots == index_ref[...]).astype(f32).astype(bf16)
    for j in range(steps):
        for i in range(1, SLOTS):
            send(i, j).wait_recv()
        arrived = back[j].reshape(SLOTS * 2 * CAP, TILE)
        for h in range(2):
            cols = pl.ds(h * HALF + j * TILE, TILE)
            picked = mm(hot[h * 256 : (h + 1) * 256], arrived)
            total = stream_ref[:, cols].astype(f32)
            total = total + picked[:128] * weight_ref[:, 0:1] + picked[128:] * weight_ref[:, 1:2]
            out_ref[:, cols] = total.astype(bf16)
    for j in range(steps):
        for i in range(1, SLOTS):
            send(i, j).wait_send()


def bring_back(hid, down, index, weight, stream):
    dma = pltpu.SemaphoreType.DMA
    steps = HALF // TILE
    vmem = pl.BlockSpec(memory_space=pltpu.VMEM)
    return pl.pallas_call(
        return_kernel,
        in_specs=[vmem, pl.BlockSpec(memory_space=pl.ANY), vmem, vmem, vmem],
        out_specs=vmem,
        out_shape=jax.ShapeDtypeStruct(stream.shape, bf16),
        scratch_shapes=[
            pltpu.VMEM((steps, 2, 4 * FFD, TILE), bf16),
            pltpu.VMEM((steps, SLOTS, 2 * CAP, TILE), bf16),
            pltpu.VMEM((steps, SLOTS, 2 * CAP, TILE), bf16),
            pltpu.VMEM((2, ROWS, TILE), bf16),
            dma((steps, 2)), dma((steps, SLOTS)), dma((steps, SLOTS)),
        ],
        compiler_params=pltpu.CompilerParams(
            collective_id=2, has_side_effects=True, vmem_limit_bytes=56 * 1024 * 1024
        ),
        name="bring_back",
    )(hid, down, index, weight, stream)


def slot_table(selected):
    z, y, core = (lax.axis_index(a) for a in SP)
    count = selected.shape[0]
    flat = selected.reshape(-1)
    member = (flat[:, None] == jnp.arange(SLOTS, dtype=jnp.int32)[None, :]).astype(jnp.int32)
    rank = jnp.sum(jnp.cumsum(member, axis=0) * member, axis=1) - 1
    away_z = (flat // 8 - z) % 4
    away_y = (flat // 2 % 4 - y) % 4
    away = (away_z * 4 + away_y) * 2 + (flat - core) % 2
    slot = jnp.zeros_like(flat)
    for i, (dz, dy, dc) in enumerate(ORDER):
        slot = slot + jnp.where(away == (dz * 4 + dy) * 2 + dc, i, 0)
    first = (slot * (2 * CAP) + rank).reshape(count, TOPK).T
    return jnp.stack([first, first + CAP])


def expert_layer(stream, normed, selected, route_weight, gate_w, lin_w, down_full):
    table = slot_table(selected)
    rows = normed.shape[0]
    slots = jnp.arange(SLOTS * 2 * CAP, dtype=jnp.int32)[:, None, None]
    hot = jnp.sum(
        (slots[..., None] == table.transpose(0, 2, 1)[None]).astype(bf16), axis=-1
    ).reshape(SLOTS * 2 * CAP, 2 * rows)
    stacked = jnp.concatenate([normed[:, :HALF], normed[:, HALF:]], axis=0)
    blocks = jnp.dot(hot, stacked, preferred_element_type=f32).astype(bf16)
    hid = dispatch(blocks.reshape(SLOTS, 2 * CAP, HALF), gate_w, lin_w)
    return bring_back(hid, down_full, table.reshape(-1, 1), route_weight, stream)


def per_device(
    queries,
    keys,
    values,
    output_gate_logits,
    decay_gate_logits,
    write_strength_logits,
    extra_log_decay,
    head_decay_rate,
    head_norm_gain,
    output_weight,
    residual,
    expert_norm_gain,
    selected_experts,
    router_chosen_scores,
    gate_up_weight,
    linear_up_weight,
    down_weight,
):
    down_full = lax.all_gather(down_weight[0], "tp", axis=0, tiled=True)
    head_mix = head_mixing(
        queries,
        keys,
        values,
        output_gate_logits,
        decay_gate_logits,
        write_strength_logits,
        extra_log_decay,
        head_decay_rate,
        head_norm_gain,
    )
    mix_sum = summed_on_arrival(
        jnp.dot(head_mix, output_weight, preferred_element_type=jnp.float32).astype(jnp.bfloat16),
        "tp",
        0,
    )
    stream = (residual.astype(jnp.float32) + mix_sum).astype(jnp.bfloat16)
    stream_wide = stream.astype(jnp.float32)
    normed = (
        stream_wide
        * lax.rsqrt(jnp.mean(stream_wide * stream_wide, axis=-1, keepdims=True) + 1e-06)
        * expert_norm_gain.astype(jnp.float32)
    ).astype(jnp.bfloat16)
    route_exp = jnp.exp(router_chosen_scores)
    route_weight = route_exp / jnp.sum(route_exp, axis=-1, keepdims=True)
    return expert_layer(
        stream, normed, selected_experts, route_weight, gate_up_weight[0], linear_up_weight[0], down_full
    )


def solution(mesh):
    torus = Mesh(mesh.devices.reshape(4, 4, 2, mesh.shape["tp"]), ("sp_0", "sp_1", "sp_2", "tp"))
    placed = (
        P(SP, "tp"),
        P(SP, "tp"),
        P(SP, "tp"),
        P(SP, "tp"),
        P(None, SP, "tp"),
        P(None, SP, "tp"),
        P(None, SP, "tp"),
        P(None, "tp"),
        P(),
        P("tp", None),
        P(SP_TP, None),
        P(),
        P(SP_TP, None),
        P(SP_TP, None),
        P(SP, None, "tp"),
        P(SP, None, "tp"),
        P(SP, "tp", None),
    )
    return jax.shard_map(
        per_device, mesh=torus, in_specs=placed, out_specs=P(SP_TP, None), check_vma=False
    )
```

```python
import jax
import jax.numpy as jnp
from jax import lax
from jax.experimental import pallas as pl
from jax.experimental.pallas import tpu as pltpu
from jax.sharding import Mesh
from jax.sharding import PartitionSpec as P

HEAD_DIM = 128
TOPK = 2
BLOCK = 128
SP = ("sp_0", "sp_1", "sp_2")
SP_TP = ("sp_0", "sp_1", "sp_2", "tp")
ARB = pltpu.CompilerParams(dimension_semantics=("arbitrary",), vmem_limit_bytes=48 * 1024 * 1024)
MESH = pl.DeviceIdType.MESH
NBLK = 4
f32 = jnp.float32
bf16 = jnp.bfloat16


def mm(a, b):
    return jnp.dot(a, b, preferred_element_type=f32)


def local_kernel(q_ref, k_ref, v_ref, ld_ref, bt_ref, out_ref, qeff_ref, blk_ref, comp_ref):
    n = BLOCK
    row = lax.broadcasted_iota(jnp.int32, (n, n), 0)
    col = lax.broadcasted_iota(jnp.int32, (n, n), 1)
    upper = (row <= col).astype(f32)
    lower = (row >= col).astype(f32)
    eye = (row == col).astype(f32)
    ld = ld_ref[0]
    highest = lax.Precision.HIGHEST
    run_f = jnp.dot(ld, upper, precision=highest, preferred_element_type=f32)
    run_b = jnp.dot(ld, lower, precision=highest, preferred_element_type=f32)
    which = lax.broadcasted_iota(jnp.int32, (2 * NBLK, n), 0)
    cum_rows = jnp.where(which < NBLK, run_f, run_b)
    cum_cols = jnp.transpose(cum_rows)
    beta_cols = jnp.transpose(bt_ref[0])
    chains = [(d, b) for d in range(2) for b in range(NBLK)]
    grams, k_un, v_un, q_un, kt_un = [], [], [], [], []
    for b in range(NBLK):
        rows = pl.ds(b * n, n)
        q = q_ref[rows, :].astype(f32)
        k = k_ref[rows, :].astype(f32)
        q = q * lax.rsqrt(jnp.sum(q * q, axis=-1, keepdims=True) + 1e-06) * HEAD_DIM ** (-0.5)
        k = k * lax.rsqrt(jnp.sum(k * k, axis=-1, keepdims=True) + 1e-06)
        kt = jnp.transpose(k).astype(bf16)
        grams.append((mm(k.astype(bf16), kt), mm(q.astype(bf16), kt)))
        q_un.append(q)
        k_un.append(k)
        kt_un.append(kt)
        v_un.append(v_ref[rows, :].astype(f32))
    low, attn, sums, pows = {}, {}, {}, {}
    for d, b in chains:
        i = d * NBLK + b
        gap = cum_cols[:, i : i + 1] - cum_rows[i : i + 1, :]
        keep = row >= col if d == 0 else row <= col
        decay = jnp.exp(jnp.where(keep, gap, -1e30))
        attn[d, b] = (grams[b][1] * decay).astype(bf16)
        strict = row > col if d == 0 else row < col
        low = jnp.where(strict, grams[b][0] * decay, 0.0) * beta_cols[:, i : i + 1]
        sums[d, b] = eye - low
        pows[d, b] = low.astype(bf16)
    for c in chains:
        pows[c] = mm(pows[c], pows[c]).astype(bf16)
    for step in range(5):
        for c in chains:
            both = mm(jnp.concatenate([sums[c].astype(bf16), pows[c]], axis=0), pows[c])
            sums[c] = sums[c] + both[:n]
            pows[c] = both[n:].astype(bf16)
    for c in chains:
        sums[c] = sums[c] + mm(sums[c].astype(bf16), pows[c])
    fresh, maps = {}, {}
    for d, b in chains:
        i = d * NBLK + b
        cc = cum_cols[:, i : i + 1]
        bt = beta_cols[:, i : i + 1]
        right = jnp.concatenate([v_un[b] * bt, k_un[b] * (-bt * jnp.exp(cc))], axis=1)
        fresh[d, b] = mm(sums[d, b].astype(bf16), right.astype(bf16))
    for d, b in chains:
        i = d * NBLK + b
        cc = cum_cols[:, i : i + 1]
        last = n - 1 if d == 0 else 0
        total = cum_rows[i : i + 1, last : last + 1]
        ended = (fresh[d, b] * jnp.exp(total - cc)).astype(bf16)
        step_map = mm(kt_un[b], ended) + jnp.concatenate(
            [jnp.zeros((n, n), f32), eye * jnp.exp(total)], axis=1
        )
        maps[d, b] = step_map
        blk_ref[0, i] = step_map.astype(bf16)
    for b in range(NBLK):
        rows = pl.ds(b * n, n)
        locals_, effs = [], []
        for d in range(2):
            i = d * NBLK + b
            given = mm(attn[d, b], fresh[d, b].astype(bf16))
            locals_.append(given[:, :n])
            effs.append(given[:, n:] + q_un[b] * jnp.exp(cum_cols[:, i : i + 1]))
        out_ref[rows, :] = locals_[0] + locals_[1]
        qeff_ref[0, rows, :] = jnp.concatenate(effs, axis=1).astype(bf16)

    def after(later, earlier):
        moved = mm(later[:, n:].astype(bf16), earlier.astype(bf16))
        return jnp.concatenate([moved[:, :n] + later[:, :n], moved[:, n:]], axis=1)

    for d in range(2):
        order = range(NBLK) if d == 0 else range(NBLK - 1, -1, -1)
        first, second, third, fourth = [maps[d, b] for b in order]
        comp_ref[0, d] = after(after(fourth, third), after(second, first)).astype(bf16)


def local_pass(queries, keys, values, log_decay, beta, heads):
    tok = queries.shape[0]
    n = BLOCK
    columns = pl.BlockSpec((tok, n), lambda h: (0, h))
    small = pl.BlockSpec((1, 2 * NBLK, n), lambda h: (h, 0, 0))
    return pl.pallas_call(
        local_kernel,
        grid=(heads,),
        in_specs=[columns, columns, columns, small, small],
        out_specs=[
            columns,
            pl.BlockSpec((1, tok, 2 * n), lambda h: (h, 0, 0)),
            pl.BlockSpec((1, 2 * NBLK, n, 2 * n), lambda h: (h, 0, 0, 0)),
            pl.BlockSpec((1, 2, n, 2 * n), lambda h: (h, 0, 0, 0)),
        ],
        out_shape=[
            jax.ShapeDtypeStruct((tok, heads * n), f32),
            jax.ShapeDtypeStruct((heads, tok, 2 * n), bf16),
            jax.ShapeDtypeStruct((heads, 2 * NBLK, n, 2 * n), bf16),
            jax.ShapeDtypeStruct((heads, 2, n, 2 * n), bf16),
        ],
        compiler_params=ARB,
        cost_estimate=pl.CostEstimate(flops=4 * 10**9, bytes_accessed=8 * 10**6, transcendentals=0),
        name="local_pass",
    )(queries, keys, values, log_decay, beta)


def exchange_kernel(
    comp_ref, down_ref, out_ref, quarter_ref,
    got, pre, chunk, start, ready, held_w, send1, recv1, send2, recv2, wsem, wsend, wrecv,
):
    n = BLOCK
    z, y, core = (lax.axis_index(a) for a in SP)
    x = lax.axis_index("tp")
    me = (z * 4 + y) * 2 + core
    depth, part = down_ref.shape[0], down_ref.shape[1] // 4
    take = pltpu.make_async_copy(
        down_ref.at[:, pl.ds(pl.multiple_of(x * part, part), part)], held_w, wsem.at[0]
    )
    take.start()
    is_owner = jnp.logical_and(core == 1, y % 2 == z % 2)
    way = y // 2
    mine = z * 2 + way

    def place(s):
        return {"sp_0": s // 8, "sp_1": (s // 2) % 4, "sp_2": s % 2}

    barrier = pltpu.get_barrier_semaphore()

    def greet(i, carry):
        other = (me + i) % 32
        pl.semaphore_signal(barrier, inc=1, device_id=place(other), device_id_type=MESH)
        return carry

    lax.fori_loop(1, 32, greet, 0)
    for dx in range(1, 4):
        pl.semaphore_signal(
            barrier, inc=1, device_id={"tp": lax.rem(x + dx, 4)}, device_id_type=MESH
        )
    pl.semaphore_wait(barrier, 34)

    def owner_of(c):
        oz = c // 2
        return (oz * 4 + (c % 2) * 2 + oz % 2) * 2 + 1

    def first_copy(c):
        return pltpu.make_async_remote_copy(
            src_ref=comp_ref.at[c],
            dst_ref=got.at[me],
            send_sem=send1.at[c],
            recv_sem=recv1.at[me],
            device_id=place(owner_of(c)),
            device_id_type=MESH,
        )

    for c in range(8):
        own = owner_of(c)

        @pl.when(me != own)
        def _():
            first_copy(c).start()

        @pl.when(me == own)
        def _():
            got[me] = comp_ref[c]

    def mine_rows(at):
        return quarter_ref.at[pl.ds(pl.multiple_of(at * depth, depth), depth), :]

    def weight_copy(dx):
        to = lax.rem(x + dx, 4)
        return pltpu.make_async_remote_copy(
            src_ref=down_ref.at[:, pl.ds(pl.multiple_of(to * part, part), part)],
            dst_ref=mine_rows(x),
            send_sem=wsend.at[dx],
            recv_sem=wrecv.at[dx],
            device_id={"tp": to},
            device_id_type=MESH,
        )

    for dx in range(1, 4):
        weight_copy(dx).start()
    take.wait()
    put = pltpu.make_async_copy(held_w, mine_rows(x), wsem.at[1])
    put.start()

    def arrival(s):
        return pltpu.make_async_remote_copy(
            src_ref=comp_ref.at[0],
            dst_ref=got.at[s],
            send_sem=send1.at[0],
            recv_sem=recv1.at[s],
            device_id=place(s),
            device_id_type=MESH,
        )

    def second_copy(p, s):
        return pltpu.make_async_remote_copy(
            src_ref=ready.at[p],
            dst_ref=out_ref.at[mine],
            send_sem=send2.at[p],
            recv_sem=recv2.at[mine],
            device_id=place(s),
            device_id_type=MESH,
        )

    @pl.when(is_owner)
    def _():
        row = lax.broadcasted_iota(jnp.int32, (n, 2 * n), 0)
        col = lax.broadcasted_iota(jnp.int32, (n, 2 * n), 1)
        unit = (row + n == col).astype(f32)
        for j in range(4):
            chunk[j] = unit

        def step(r, carry):
            for j in range(4):
                p = 8 * j + r
                s = p + way * (31 - 2 * p)

                @pl.when(s != me)
                def _():
                    arrival(s).wait_recv()

                now = chunk[j].astype(bf16)
                pre[p] = now
                moved = mm(got[s, :, n:], now)
                chunk[j, :, :n] = moved[:, :n] + got[s, :, :n].astype(f32)
                chunk[j, :, n:] = moved[:, n:]
            return carry

        lax.fori_loop(0, 8, step, 0)
        start[0] = jnp.zeros((n, n), bf16)
        held = jnp.zeros((n, n), f32)
        for j in range(3):
            held = mm(chunk[j, :, n:].astype(bf16), held.astype(bf16)) + chunk[j, :, :n]
            start[j + 1] = held.astype(bf16)

        def finish(r, carry):
            for j in range(4):
                p = 8 * j + r
                s = p + way * (31 - 2 * p)
                given = mm(pre[p, :, n:], start[j]) + pre[p, :, :n].astype(f32)
                ready[p] = given.astype(bf16)

                @pl.when(s != me)
                def _():
                    second_copy(p, s).start()

                @pl.when(s == me)
                def _():
                    out_ref[mine] = given.astype(bf16)

            return carry

        lax.fori_loop(0, 8, finish, 0)

        def drain(p, carry):
            s = p + way * (31 - 2 * p)

            @pl.when(s != me)
            def _():
                second_copy(p, s).wait_send()

            return carry

        lax.fori_loop(0, 32, drain, 0)

    for c in range(8):

        @pl.when(me != owner_of(c))
        def _():
            first_copy(c).wait_send()
            pltpu.make_async_remote_copy(
                src_ref=ready.at[0],
                dst_ref=out_ref.at[c],
                send_sem=send2.at[0],
                recv_sem=recv2.at[c],
                device_id=place(owner_of(c)),
                device_id_type=MESH,
            ).wait_recv()

    put.wait()
    for dx in range(1, 4):
        weight_copy(dx).wait_send()
        pltpu.make_async_remote_copy(
            src_ref=down_ref.at[:, pl.ds(0, part)],
            dst_ref=mine_rows(lax.rem(x + 4 - dx, 4)),
            send_sem=wsend.at[dx],
            recv_sem=wrecv.at[dx],
            device_id={"tp": lax.rem(x + 4 - dx, 4)},
            device_id_type=MESH,
        ).wait_recv()


def exchange(comp, down):
    n = BLOCK
    depth, part = down.shape[0], down.shape[1] // 4
    return pl.pallas_call(
        exchange_kernel,
        in_specs=[pl.BlockSpec(memory_space=pltpu.VMEM), pl.BlockSpec(memory_space=pl.ANY)],
        out_specs=[pl.BlockSpec(memory_space=pltpu.VMEM), pl.BlockSpec(memory_space=pl.ANY)],
        out_shape=[
            jax.ShapeDtypeStruct((8, n, n), bf16),
            jax.ShapeDtypeStruct((4 * depth, part), bf16),
        ],
        scratch_shapes=[
            pltpu.VMEM((32, n, 2 * n), bf16),
            pltpu.VMEM((32, n, 2 * n), bf16),
            pltpu.VMEM((4, n, 2 * n), f32),
            pltpu.VMEM((4, n, n), bf16),
            pltpu.VMEM((32, n, n), bf16),
            pltpu.VMEM((depth, part), bf16),
            pltpu.SemaphoreType.DMA((8,)),
            pltpu.SemaphoreType.DMA((32,)),
            pltpu.SemaphoreType.DMA((32,)),
            pltpu.SemaphoreType.DMA((8,)),
            pltpu.SemaphoreType.DMA((2,)),
            pltpu.SemaphoreType.DMA((4,)),
            pltpu.SemaphoreType.DMA((4,)),
        ],
        compiler_params=pltpu.CompilerParams(collective_id=0, has_side_effects=True),
        cost_estimate=pl.CostEstimate(flops=9 * 10**9, bytes_accessed=8 * 10**6, transcendentals=0),
        name="exchange",
    )(comp, down)


def finish_kernel(out_ref, qeff_ref, blk_ref, sin_ref, gate_ref, gain_ref, mix_ref):
    n = BLOCK
    gain = gain_ref[...].astype(f32)
    states = {}
    held = [sin_ref[0, d].astype(f32) for d in range(2)]
    for step in range(NBLK):
        for d in range(2):
            b = step if d == 0 else NBLK - 1 - step
            states[d, b] = held[d].astype(bf16)
            if step < NBLK - 1:
                i = d * NBLK + b
                held[d] = mm(blk_ref[0, i, :, n:], states[d, b]) + blk_ref[0, i, :, :n].astype(f32)
    for b in range(NBLK):
        rows = pl.ds(b * n, n)
        both = jnp.concatenate([states[0, b], states[1, b]], axis=0)
        o = out_ref[rows, :] + mm(qeff_ref[0, rows, :], both)
        o = o * lax.rsqrt(jnp.mean(o * o, axis=-1, keepdims=True) + 1e-06) * gain
        g = gate_ref[rows, :].astype(f32)
        mix_ref[rows, :] = (o * (g * jax.nn.sigmoid(g))).astype(bf16)


def finish_pass(out_local, qeff, blk, entering, gates, gain):
    tok, width = out_local.shape
    n = BLOCK
    heads = width // n
    columns = pl.BlockSpec((tok, n), lambda h: (0, h))
    return pl.pallas_call(
        finish_kernel,
        grid=(heads,),
        in_specs=[
            columns,
            pl.BlockSpec((1, tok, 2 * n), lambda h: (h, 0, 0)),
            pl.BlockSpec((1, 2 * NBLK, n, 2 * n), lambda h: (h, 0, 0, 0)),
            pl.BlockSpec((1, 2, n, n), lambda h: (h, 0, 0, 0)),
            columns,
            pl.BlockSpec((1, n), lambda h: (0, 0)),
        ],
        out_specs=columns,
        out_shape=jax.ShapeDtypeStruct((tok, width), bf16),
        compiler_params=ARB,
        name="finish_pass",
    )(out_local, qeff, blk, entering, gates, gain)


def swap_kernel(mix_ref, out_ref, own_sem, send, recv):
    x = lax.axis_index("tp")
    rows, part = mix_ref.shape[0] // 4, mix_ref.shape[1]
    barrier = pltpu.get_barrier_semaphore()
    for dx in range(1, 4):
        pl.semaphore_signal(
            barrier, inc=1, device_id={"tp": lax.rem(x + dx, 4)}, device_id_type=MESH
        )
    pl.semaphore_wait(barrier, 3)

    def rows_of(at):
        return mix_ref.at[pl.ds(pl.multiple_of(at * rows, rows), rows), :]

    def place_of(half, at):
        return out_ref.at[
            pl.ds(half * rows, rows), pl.ds(pl.multiple_of(at * part, part), part)
        ]

    def copy(half, dx, back):
        to = lax.rem(x + (4 - dx if back else dx), 4)
        return pltpu.make_async_remote_copy(
            src_ref=rows_of(lax.rem(to + 2 * half, 4)), dst_ref=place_of(half, to if back else x),
            send_sem=send.at[half, dx], recv_sem=recv.at[half, dx], device_id={"tp": to},
            device_id_type=MESH,
        )

    for dx in (2, 1, 3):
        for half in range(2):
            copy(half, dx, False).start()
    for half in range(2):
        own = pltpu.make_async_copy(
            rows_of(lax.rem(x + 2 * half, 4)), place_of(half, x), own_sem.at[half]
        )
        own.start()
        own.wait()
    for dx in (1, 3, 2):
        for half in range(2):
            copy(half, dx, False).wait_send()
            copy(half, dx, True).wait_recv()


def swap(mix):
    dma = pltpu.SemaphoreType.DMA
    return pl.pallas_call(
        swap_kernel,
        in_specs=[pl.BlockSpec(memory_space=pltpu.VMEM)],
        out_specs=pl.BlockSpec(memory_space=pltpu.VMEM),
        out_shape=jax.ShapeDtypeStruct((mix.shape[0] // 2, mix.shape[1] * 4), bf16),
        scratch_shapes=[dma((2,)), dma((2, 4)), dma((2, 4))],
        compiler_params=pltpu.CompilerParams(collective_id=3, has_side_effects=True),
        name="swap",
    )(mix)


def head_mixing(queries, keys, values, gates, decay_logits, write_logits, extra, rate, gain, down):
    tok, width = queries.shape
    heads = width // HEAD_DIM
    log_decay = -rate[:, None, :] * jax.nn.softplus(decay_logits) + extra
    beta = jax.nn.sigmoid(write_logits)

    def per_head(t):
        t = t.transpose(2, 0, 1).reshape(heads, 2 * NBLK, BLOCK)
        return t

    out_local, qeff, blk, comp = local_pass(
        queries, keys, values, per_head(log_decay), per_head(beta), heads
    )
    entering, down_quarter = exchange(comp.reshape(2 * heads, BLOCK, 2 * BLOCK), down)
    mix = finish_pass(
        out_local, qeff, blk, entering.reshape(heads, 2, BLOCK, BLOCK), gates, gain.reshape(1, -1)
    )
    return swap(mix), down_quarter


ORDER = (
    (0, 0, 0), (2, 2, 1), (0, 0, 1), (2, 2, 0), (0, 1, 0), (2, 3, 1), (0, 1, 1), (2, 3, 0),
    (1, 0, 0), (2, 1, 1), (1, 0, 1), (2, 1, 0), (0, 3, 0), (3, 2, 1), (0, 3, 1), (3, 2, 0),
    (3, 0, 0), (1, 2, 1), (3, 0, 1), (1, 2, 0), (1, 1, 0), (2, 0, 1), (1, 1, 1), (2, 0, 0),
    (3, 3, 0), (0, 2, 1), (3, 3, 1), (0, 2, 0), (1, 3, 0), (3, 1, 1), (1, 3, 1), (3, 1, 0),
)
CAP = 12
TILE = 512
AHEAD = 8
SLOTS = len(ORDER)
HALF = 2048
FFD = 384
ROWS = SLOTS * CAP


def plane_place(z, y, core, offset, sign):
    dz, dy, dc = offset
    return {
        "sp_0": lax.rem(z + (dz if sign > 0 else 4 - dz), 4),
        "sp_1": lax.rem(y + (dy if sign > 0 else 4 - dy), 4),
        "sp_2": lax.rem(core + dc, 2),
    }


def dispatch_kernel(
    blocks_ref, gate_ref, lin_ref, down_ref, index_ref, weight_ref, stream_ref, out_ref,
    xb, wg, wl, act_buf, hid_ref, wd, ready, back,
    wsem, send0, send1, recv, hsend, rsend, hrecv, hfar, sends, recvs,
):
    z, y, core = (lax.axis_index(a) for a in SP)
    x = lax.axis_index("tp")
    right, left, far = lax.rem(x + 1, 4), lax.rem(x + 3, 4), lax.rem(x + 2, 4)
    keep = pltpu.make_async_copy(blocks_ref.at[0], xb.at[0, 0], wsem.at[2])
    keep.start()
    load_g = pltpu.make_async_copy(gate_ref, wg, wsem.at[0])
    load_l = pltpu.make_async_copy(lin_ref, wl, wsem.at[1])
    load_g.start()
    load_l.start()
    load_d = pltpu.make_async_copy(down_ref, wd, wsem.at[3])
    load_d.start()
    barrier = pltpu.get_barrier_semaphore()
    for dx in range(4):
        for offset in ORDER:
            if dx or offset != ORDER[0]:
                to = plane_place(z, y, core, offset, 1)
                to["tp"] = lax.rem(x + dx, 4)
                pl.semaphore_signal(barrier, inc=1, device_id=to, device_id_type=MESH)
    pl.semaphore_wait(barrier, 4 * SLOTS - 1)

    def plane_copy(i):
        return pltpu.make_async_remote_copy(
            src_ref=blocks_ref.at[i], dst_ref=xb.at[0, i], send_sem=send0.at[i],
            recv_sem=recv.at[0, i], device_id=plane_place(z, y, core, ORDER[i], 1),
            device_id_type=MESH,
        )

    def line_copy(i, to):
        return pltpu.make_async_remote_copy(
            src_ref=xb.at[0, i], dst_ref=xb.at[1, i], send_sem=send1.at[i],
            recv_sem=recv.at[1, i], device_id={"tp": to}, device_id_type=MESH,
        )

    def arrival(pair, i):
        return pltpu.make_async_remote_copy(
            src_ref=blocks_ref.at[0], dst_ref=xb.at[pair, i], send_sem=send0.at[0],
            recv_sem=recv.at[pair, i], device_id={"tp": right}, device_id_type=MESH,
        )

    for i in range(1, AHEAD + 1):
        plane_copy(i).start()
    keep.wait()
    r = lax.broadcasted_iota(jnp.int32, (192, 192), 0)
    c = lax.broadcasted_iota(jnp.int32, (192, 192), 1)
    within = lax.rem(r, 96)
    source = (within // CAP) * (2 * CAP) + (r // 96) * CAP + lax.rem(within, CAP)
    perm = (c == source).astype(f32).astype(bf16)
    source_2 = (lax.rem(r, 2 * CAP) // CAP) * 96 + (r // (2 * CAP)) * CAP + lax.rem(
        lax.rem(r, 2 * CAP), CAP
    )
    perm_2 = (c == source_2).astype(f32).astype(bf16)
    parity = lax.rem(x, 2)
    load_g.wait()
    load_l.wait()
    load_d.wait()

    def compute(pair, part):
        rows = xb[pair, pl.ds(part * 8, 8)].reshape(192, 2 * HALF)
        gate = jnp.minimum(mm(rows, wg[...]), 7.0)
        lin = mm(rows, wl[...])
        act = gate * jax.nn.sigmoid(1.702 * gate) * (jnp.clip(lin, -7.0, 7.0) + 1.0)
        fixed = mm(perm, act.astype(bf16)).astype(bf16)
        low = parity if pair == 0 else 1 - parity
        for half in range(2):
            piece = fixed[half * 96 : (half + 1) * 96]
            act_buf[part, low + 2 * half] = piece
            hid_ref[part, x, low + 2 * half] = piece

    def hid_copy(part, way):
        return pltpu.make_async_remote_copy(
            src_ref=act_buf.at[part], dst_ref=hid_ref.at[part, x],
            send_sem=hsend.at[part, way], recv_sem=hrecv.at[part, x],
            device_id={"tp": lax.rem(x + way, 4)}, device_id_type=MESH,
        )

    def hid_arrival(part, piece):
        return pltpu.make_async_remote_copy(
            src_ref=act_buf.at[part], dst_ref=hid_ref.at[part, piece],
            send_sem=hsend.at[part, 1], recv_sem=hrecv.at[part, piece],
            device_id={"tp": right}, device_id_type=MESH,
        )

    def hid_relay(part, half, piece, to):
        here = hid_ref.at[part, piece, pl.ds(2 * half, 2)]
        return pltpu.make_async_remote_copy(
            src_ref=here, dst_ref=here, send_sem=rsend.at[part, half],
            recv_sem=hfar.at[part, half], device_id={"tp": to}, device_id_type=MESH,
        )

    def relay(part):
        hid_arrival(part, left).wait_recv()
        hid_relay(part, 0, left, right).start()
        hid_arrival(part, right).wait_recv()
        hid_relay(part, 1, right, left).start()

    def send(i, dx):
        to = plane_place(z, y, core, ORDER[i], -1)
        to["tp"] = lax.rem(x + dx, 4)
        return pltpu.make_async_remote_copy(
            src_ref=ready.at[dx, i], dst_ref=back.at[x, i], send_sem=sends.at[dx, i],
            recv_sem=recvs.at[x, i], device_id=to, device_id_type=MESH,
        )

    def project(part):
        totals = []
        for h in range(2):
            cols = pl.ds(h * TILE, TILE)
            total = mm(hid_ref[part, 0].reshape(ROWS, FFD), wd[pl.ds(0, FFD), cols])
            for k in range(1, 4):
                piece = hid_ref[part, k].reshape(ROWS, FFD)
                total = total + mm(piece, wd[pl.ds(k * FFD, FFD), cols])
            totals.append(total.astype(bf16))
        for group in range(4):
            rows = slice(group * 96, (group + 1) * 96)
            both = jnp.concatenate([totals[0][rows], totals[1][rows]], axis=0)
            mixed = mm(perm_2, both).astype(bf16).reshape(8, 2 * CAP, TILE)
            ready[lax.rem(group + 4 - x, 4), pl.ds(part * 8, 8)] = mixed
        for q in range(4):

            @pl.when(part == q)
            def _():
                for i in range(8 * q, 8 * q + 8):
                    for dx in (2, 1, 3, 0):
                        if i or dx:
                            send(i, dx).start()

    def turn(part, carry):
        for p in range(4):

            @pl.when(part == p)
            def _():
                for i in range(8 * p, 8 * p + 8):
                    if i:
                        if i + AHEAD < SLOTS:
                            plane_copy(i).wait_send()
                            plane_copy(i + AHEAD).start()
                        arrival(0, i).wait_recv()
                    line_copy(i, left if i % 2 else right).start()

        @pl.when(part > 0)
        def _():
            relay(part - 1)

        @pl.when(part < 4)
        def _():
            compute(0, part)

            def landed(j, carry):
                arrival(1, part * 8 + j).wait_recv()
                return carry

            lax.fori_loop(0, 8, landed, 0)
            compute(1, part)
            hid_copy(part, 1).start()
            hid_copy(part, 3).start()

        @pl.when(part > 0)
        def _():
            for half in range(2):
                hid_relay(part - 1, half, far, right).wait_recv()
            project(part - 1)

        return carry

    lax.fori_loop(0, 5, turn, 0)
    back[x, 0] = ready[0, 0]
    slots = lax.broadcasted_iota(jnp.int32, (512, SLOTS * 2 * CAP), 1)
    hot = (slots == index_ref[...]).astype(f32).astype(bf16)
    for dx in (0, 1, 3, 2):
        piece = lax.rem(x + dx, 4)
        for i in range(SLOTS):
            if i or dx:
                pltpu.make_async_remote_copy(
                    src_ref=ready.at[0, 0], dst_ref=back.at[piece, i], send_sem=sends.at[0, 0],
                    recv_sem=recvs.at[piece, i], device_id={"tp": right},
                    device_id_type=MESH,
                ).wait_recv()
        arrived = back[piece].reshape(SLOTS * 2 * CAP, TILE)
        for h in range(2):
            cols = pl.ds(pl.multiple_of(piece * (2 * TILE) + h * TILE, TILE), TILE)
            picked = mm(hot[h * 256 : (h + 1) * 256], arrived)
            total = stream_ref[:, cols].astype(f32)
            total = total + picked[:128] * weight_ref[:, 0:1] + picked[128:] * weight_ref[:, 1:2]
            out_ref[:, cols] = total.astype(bf16)

    def finish(part, carry):
        for half in range(2):
            hid_relay(part, half, far, right).wait_send()
        hid_copy(part, 1).wait_send()
        hid_copy(part, 3).wait_send()
        return carry

    lax.fori_loop(0, 4, finish, 0)
    for i in range(SLOTS):
        if i + AHEAD >= SLOTS:
            plane_copy(i).wait_send()
        line_copy(i, right).wait_send()
        for dx in range(4):
            if i or dx:
                send(i, dx).wait_send()


def dispatch(blocks, gate_w, lin_w, down, index, weight, stream):
    width = gate_w.shape[0]
    dma = pltpu.SemaphoreType.DMA
    vmem, far_off = (pl.BlockSpec(memory_space=m) for m in (pltpu.VMEM, pl.ANY))
    return pl.pallas_call(
        dispatch_kernel,
        in_specs=[vmem, far_off, far_off, far_off, vmem, vmem, vmem],
        out_specs=vmem,
        out_shape=jax.ShapeDtypeStruct(stream.shape, bf16),
        scratch_shapes=[
            pltpu.VMEM((2, SLOTS, 2 * CAP, width), bf16),
            pltpu.VMEM((width, FFD), bf16),
            pltpu.VMEM((width, FFD), bf16),
            pltpu.VMEM((4, 4, 96, FFD), bf16),
            pltpu.VMEM((4, 4, 4, 96, FFD), bf16),
            pltpu.VMEM(down.shape, bf16),
            pltpu.VMEM((4, SLOTS, 2 * CAP, TILE), bf16),
            pltpu.VMEM((4, SLOTS, 2 * CAP, TILE), bf16),
            dma((4,)), dma((SLOTS,)), dma((SLOTS,)), dma((2, SLOTS)),
            dma((4, 4)), dma((4, 2)), dma((4, 4)), dma((4, 2)), dma((4, SLOTS)), dma((4, SLOTS)),
        ],
        compiler_params=pltpu.CompilerParams(
            collective_id=1, has_side_effects=True, vmem_limit_bytes=58 * 1024 * 1024
        ),
        name="experts",
    )(blocks, gate_w, lin_w, down, index, weight, stream)


def slot_table(selected):
    z, y, core = (lax.axis_index(a) for a in SP)
    count = selected.shape[0]
    flat = selected.reshape(-1)
    member = (flat[:, None] == jnp.arange(SLOTS, dtype=jnp.int32)[None, :]).astype(jnp.int32)
    rank = jnp.sum(jnp.cumsum(member, axis=0) * member, axis=1) - 1
    away_z = (flat // 8 - z) % 4
    away_y = (flat // 2 % 4 - y) % 4
    away = (away_z * 4 + away_y) * 2 + (flat - core) % 2
    slot = jnp.zeros_like(flat)
    for i, (dz, dy, dc) in enumerate(ORDER):
        slot = slot + jnp.where(away == (dz * 4 + dy) * 2 + dc, i, 0)
    return slot.reshape(count, TOPK), rank.reshape(count, TOPK)


def expert_layer(stream, normed, selected, other, route_weight, gate_w, lin_w, down_quarter):
    rows = selected.shape[0]
    late = lax.axis_index("tp") // 2
    slot, rank = slot_table(selected)
    first = slot * (2 * CAP) + rank
    table = jnp.stack([first.T, first.T + CAP])
    slot_2, rank_2 = slot_table(other)
    source = jnp.concatenate(
        [first + late * CAP, slot_2 * (2 * CAP) + rank_2 + (1 - late) * CAP], axis=0
    )
    slots = jnp.arange(SLOTS * 2 * CAP, dtype=jnp.int32)[:, None]
    hot = (slots == source[None, :, 0]).astype(bf16) + (slots == source[None, :, 1]).astype(bf16)
    blocks = jnp.dot(hot, normed, preferred_element_type=f32).astype(bf16)
    return dispatch(
        blocks.reshape(SLOTS, 2 * CAP, 2 * HALF),
        gate_w,
        lin_w,
        down_quarter,
        table.reshape(4 * rows, 1),
        route_weight,
        stream,
    )


def per_device(
    queries,
    keys,
    values,
    output_gate_logits,
    decay_gate_logits,
    write_strength_logits,
    extra_log_decay,
    head_decay_rate,
    head_norm_gain,
    output_weight,
    residual,
    expert_norm_gain,
    selected_experts,
    router_chosen_scores,
    gate_up_weight,
    linear_up_weight,
    down_weight,
):
    place = (lax.axis_index("sp_0") * 4 + lax.axis_index("sp_1")) * 2 + lax.axis_index("sp_2")
    few = output_weight.shape[0] // lax.axis_size(SP)
    own_rows = lax.dynamic_slice_in_dim(output_weight, place * few, few, axis=0)
    full_weight = lax.all_gather(own_rows, ("tp",) + SP, axis=0, tiled=True)
    opposite = [(i, (i + 2) % 4) for i in range(4)]
    residual_2 = lax.ppermute(residual, "tp", opposite)
    selected_2 = lax.ppermute(selected_experts, "tp", opposite)
    head_mix, down_quarter = head_mixing(
        queries,
        keys,
        values,
        output_gate_logits,
        decay_gate_logits,
        write_strength_logits,
        extra_log_decay,
        head_decay_rate,
        head_norm_gain,
        down_weight[0],
    )
    mix_sum = jnp.dot(head_mix, full_weight, preferred_element_type=jnp.float32)
    both = jnp.concatenate([residual, residual_2], axis=0)
    stream = (both.astype(jnp.float32) + mix_sum).astype(jnp.bfloat16)
    stream_wide = stream.astype(jnp.float32)
    normed = (
        stream_wide
        * lax.rsqrt(jnp.mean(stream_wide * stream_wide, axis=-1, keepdims=True) + 1e-06)
        * expert_norm_gain.astype(jnp.float32)
    ).astype(jnp.bfloat16)
    route_exp = jnp.exp(router_chosen_scores)
    route_weight = route_exp / jnp.sum(route_exp, axis=-1, keepdims=True)
    return expert_layer(
        stream[: residual.shape[0]],
        normed,
        selected_experts,
        selected_2,
        route_weight,
        gate_up_weight[0],
        linear_up_weight[0],
        down_quarter,
    )


def solution(mesh):
    torus = Mesh(mesh.devices.reshape(4, 4, 2, mesh.shape["tp"]), ("sp_0", "sp_1", "sp_2", "tp"))
    placed = (
        P(SP, "tp"),
        P(SP, "tp"),
        P(SP, "tp"),
        P(SP, "tp"),
        P(None, SP, "tp"),
        P(None, SP, "tp"),
        P(None, SP, "tp"),
        P(None, "tp"),
        P(),
        P("tp", None),
        P(SP_TP, None),
        P(),
        P(SP_TP, None),
        P(SP_TP, None),
        P(SP, None, "tp"),
        P(SP, None, "tp"),
        P(SP, "tp", None),
    )
    return jax.shard_map(
        per_device, mesh=torus, in_specs=placed, out_specs=P(SP_TP, None), check_vma=False
    )
```

```python
import jax
import jax.numpy as jnp
from jax import lax
from jax.experimental import pallas as pl
from jax.experimental.pallas import tpu as pltpu
from jax.sharding import Mesh
from jax.sharding import PartitionSpec as P

HEAD_DIM = 128
TOPK = 2
BLOCK = 128
SP = ("sp_0", "sp_1", "sp_2")
SP_TP = ("sp_0", "sp_1", "sp_2", "tp")
ARB = pltpu.CompilerParams(dimension_semantics=("arbitrary",), vmem_limit_bytes=48 * 1024 * 1024)
MESH = pl.DeviceIdType.MESH
NBLK = 4
f32 = jnp.float32
bf16 = jnp.bfloat16


def mm(a, b):
    return jnp.dot(a, b, preferred_element_type=f32)


def local_kernel(q_ref, k_ref, v_ref, ld_ref, bt_ref, out_ref, qeff_ref, blk_ref, comp_ref):
    n = BLOCK
    row = lax.broadcasted_iota(jnp.int32, (n, n), 0)
    col = lax.broadcasted_iota(jnp.int32, (n, n), 1)
    upper = (row <= col).astype(f32)
    lower = (row >= col).astype(f32)
    eye = (row == col).astype(f32)
    ld = ld_ref[0]
    highest = lax.Precision.HIGHEST
    run_f = jnp.dot(ld, upper, precision=highest, preferred_element_type=f32)
    run_b = jnp.dot(ld, lower, precision=highest, preferred_element_type=f32)
    which = lax.broadcasted_iota(jnp.int32, (2 * NBLK, n), 0)
    cum_rows = jnp.where(which < NBLK, run_f, run_b)
    cum_cols = jnp.transpose(cum_rows)
    beta_cols = jnp.transpose(bt_ref[0])
    chains = [(d, b) for d in range(2) for b in range(NBLK)]
    grams, k_un, v_un, q_un, kt_un = [], [], [], [], []
    for b in range(NBLK):
        rows = pl.ds(b * n, n)
        q = q_ref[rows, :].astype(f32)
        k = k_ref[rows, :].astype(f32)
        q = q * lax.rsqrt(jnp.sum(q * q, axis=-1, keepdims=True) + 1e-06) * HEAD_DIM ** (-0.5)
        k = k * lax.rsqrt(jnp.sum(k * k, axis=-1, keepdims=True) + 1e-06)
        kt = jnp.transpose(k).astype(bf16)
        grams.append((mm(k.astype(bf16), kt), mm(q.astype(bf16), kt)))
        q_un.append(q)
        k_un.append(k)
        kt_un.append(kt)
        v_un.append(v_ref[rows, :].astype(f32))
    low, attn, sums, pows = {}, {}, {}, {}
    for d, b in chains:
        i = d * NBLK + b
        gap = cum_cols[:, i : i + 1] - cum_rows[i : i + 1, :]
        keep = row >= col if d == 0 else row <= col
        decay = jnp.exp(jnp.where(keep, gap, -1e30))
        attn[d, b] = (grams[b][1] * decay).astype(bf16)
        strict = row > col if d == 0 else row < col
        low = jnp.where(strict, grams[b][0] * decay, 0.0) * beta_cols[:, i : i + 1]
        sums[d, b] = eye - low
        pows[d, b] = low.astype(bf16)
    for c in chains:
        pows[c] = mm(pows[c], pows[c]).astype(bf16)
    for step in range(5):
        for c in chains:
            both = mm(jnp.concatenate([sums[c].astype(bf16), pows[c]], axis=0), pows[c])
            sums[c] = sums[c] + both[:n]
            pows[c] = both[n:].astype(bf16)
    for c in chains:
        sums[c] = sums[c] + mm(sums[c].astype(bf16), pows[c])
    fresh, maps = {}, {}
    for d, b in chains:
        i = d * NBLK + b
        cc = cum_cols[:, i : i + 1]
        bt = beta_cols[:, i : i + 1]
        right = jnp.concatenate([v_un[b] * bt, k_un[b] * (-bt * jnp.exp(cc))], axis=1)
        fresh[d, b] = mm(sums[d, b].astype(bf16), right.astype(bf16))
    for d, b in chains:
        i = d * NBLK + b
        cc = cum_cols[:, i : i + 1]
        last = n - 1 if d == 0 else 0
        total = cum_rows[i : i + 1, last : last + 1]
        ended = (fresh[d, b] * jnp.exp(total - cc)).astype(bf16)
        step_map = mm(kt_un[b], ended) + jnp.concatenate(
            [jnp.zeros((n, n), f32), eye * jnp.exp(total)], axis=1
        )
        maps[d, b] = step_map
        blk_ref[0, i] = step_map.astype(bf16)
    for b in range(NBLK):
        rows = pl.ds(b * n, n)
        locals_, effs = [], []
        for d in range(2):
            i = d * NBLK + b
            given = mm(attn[d, b], fresh[d, b].astype(bf16))
            locals_.append(given[:, :n])
            effs.append(given[:, n:] + q_un[b] * jnp.exp(cum_cols[:, i : i + 1]))
        out_ref[rows, :] = locals_[0] + locals_[1]
        qeff_ref[0, rows, :] = jnp.concatenate(effs, axis=1).astype(bf16)

    def after(later, earlier):
        moved = mm(later[:, n:].astype(bf16), earlier.astype(bf16))
        return jnp.concatenate([moved[:, :n] + later[:, :n], moved[:, n:]], axis=1)

    for d in range(2):
        order = range(NBLK) if d == 0 else range(NBLK - 1, -1, -1)
        first, second, third, fourth = [maps[d, b] for b in order]
        comp_ref[0, d] = after(after(fourth, third), after(second, first)).astype(bf16)


def local_pass(queries, keys, values, log_decay, beta, heads):
    tok = queries.shape[0]
    n = BLOCK
    columns = pl.BlockSpec((tok, n), lambda h: (0, h))
    small = pl.BlockSpec((1, 2 * NBLK, n), lambda h: (h, 0, 0))
    return pl.pallas_call(
        local_kernel,
        grid=(heads,),
        in_specs=[columns, columns, columns, small, small],
        out_specs=[
            columns,
            pl.BlockSpec((1, tok, 2 * n), lambda h: (h, 0, 0)),
            pl.BlockSpec((1, 2 * NBLK, n, 2 * n), lambda h: (h, 0, 0, 0)),
            pl.BlockSpec((1, 2, n, 2 * n), lambda h: (h, 0, 0, 0)),
        ],
        out_shape=[
            jax.ShapeDtypeStruct((tok, heads * n), f32),
            jax.ShapeDtypeStruct((heads, tok, 2 * n), bf16),
            jax.ShapeDtypeStruct((heads, 2 * NBLK, n, 2 * n), bf16),
            jax.ShapeDtypeStruct((heads, 2, n, 2 * n), bf16),
        ],
        compiler_params=ARB,
        cost_estimate=pl.CostEstimate(flops=4 * 10**9, bytes_accessed=8 * 10**6, transcendentals=0),
        name="local_pass",
    )(queries, keys, values, log_decay, beta)


def exchange_kernel(
    comp_ref, down_ref, out_ref, quarter_ref,
    got, pre, chunk, start, ready, held_w, send1, recv1, send2, recv2, wsem, wsend, wrecv,
):
    n = BLOCK
    z, y, core = (lax.axis_index(a) for a in SP)
    x = lax.axis_index("tp")
    me = (z * 4 + y) * 2 + core
    depth, part = down_ref.shape[0], down_ref.shape[1] // 4
    take = pltpu.make_async_copy(
        down_ref.at[:, pl.ds(pl.multiple_of(x * part, part), part)], held_w, wsem.at[0]
    )
    take.start()
    is_owner = jnp.logical_and(core == 1, y % 2 == z % 2)
    way = y // 2
    mine = z * 2 + way

    def place(s):
        return {"sp_0": s // 8, "sp_1": (s // 2) % 4, "sp_2": s % 2}

    barrier = pltpu.get_barrier_semaphore()

    def greet(i, carry):
        other = (me + i) % 32
        pl.semaphore_signal(barrier, inc=1, device_id=place(other), device_id_type=MESH)
        return carry

    lax.fori_loop(1, 32, greet, 0)
    for dx in range(1, 4):
        pl.semaphore_signal(
            barrier, inc=1, device_id={"tp": lax.rem(x + dx, 4)}, device_id_type=MESH
        )
    pl.semaphore_wait(barrier, 34)

    def owner_of(c):
        oz = c // 2
        return (oz * 4 + (c % 2) * 2 + oz % 2) * 2 + 1

    def first_copy(c):
        return pltpu.make_async_remote_copy(
            src_ref=comp_ref.at[c],
            dst_ref=got.at[me],
            send_sem=send1.at[c],
            recv_sem=recv1.at[me],
            device_id=place(owner_of(c)),
            device_id_type=MESH,
        )

    for c in range(8):
        own = owner_of(c)

        @pl.when(me != own)
        def _():
            first_copy(c).start()

        @pl.when(me == own)
        def _():
            got[me] = comp_ref[c]

    def mine_rows(at):
        return quarter_ref.at[pl.ds(pl.multiple_of(at * depth, depth), depth), :]

    def weight_copy(dx):
        to = lax.rem(x + dx, 4)
        return pltpu.make_async_remote_copy(
            src_ref=down_ref.at[:, pl.ds(pl.multiple_of(to * part, part), part)],
            dst_ref=mine_rows(x),
            send_sem=wsend.at[dx],
            recv_sem=wrecv.at[dx],
            device_id={"tp": to},
            device_id_type=MESH,
        )

    for dx in range(1, 4):
        weight_copy(dx).start()
    take.wait()
    put = pltpu.make_async_copy(held_w, mine_rows(x), wsem.at[1])
    put.start()

    def arrival(s):
        return pltpu.make_async_remote_copy(
            src_ref=comp_ref.at[0],
            dst_ref=got.at[s],
            send_sem=send1.at[0],
            recv_sem=recv1.at[s],
            device_id=place(s),
            device_id_type=MESH,
        )

    def second_copy(p, s):
        return pltpu.make_async_remote_copy(
            src_ref=ready.at[p],
            dst_ref=out_ref.at[mine],
            send_sem=send2.at[p],
            recv_sem=recv2.at[mine],
            device_id=place(s),
            device_id_type=MESH,
        )

    @pl.when(is_owner)
    def _():
        row = lax.broadcasted_iota(jnp.int32, (n, 2 * n), 0)
        col = lax.broadcasted_iota(jnp.int32, (n, 2 * n), 1)
        unit = (row + n == col).astype(f32)
        for j in range(4):
            chunk[j] = unit

        def step(r, carry):
            for j in range(4):
                p = 8 * j + r
                s = p + way * (31 - 2 * p)

                @pl.when(s != me)
                def _():
                    arrival(s).wait_recv()

                now = chunk[j].astype(bf16)
                pre[p] = now
                moved = mm(got[s, :, n:], now)
                chunk[j, :, :n] = moved[:, :n] + got[s, :, :n].astype(f32)
                chunk[j, :, n:] = moved[:, n:]
            return carry

        lax.fori_loop(0, 8, step, 0)
        start[0] = jnp.zeros((n, n), bf16)
        held = jnp.zeros((n, n), f32)
        for j in range(3):
            held = mm(chunk[j, :, n:].astype(bf16), held.astype(bf16)) + chunk[j, :, :n]
            start[j + 1] = held.astype(bf16)

        def finish(r, carry):
            for j in range(4):
                p = 8 * j + r
                s = p + way * (31 - 2 * p)
                given = mm(pre[p, :, n:], start[j]) + pre[p, :, :n].astype(f32)
                ready[p] = given.astype(bf16)

                @pl.when(s != me)
                def _():
                    second_copy(p, s).start()

                @pl.when(s == me)
                def _():
                    out_ref[mine] = given.astype(bf16)

            return carry

        lax.fori_loop(0, 8, finish, 0)

        def drain(p, carry):
            s = p + way * (31 - 2 * p)

            @pl.when(s != me)
            def _():
                second_copy(p, s).wait_send()

            return carry

        lax.fori_loop(0, 32, drain, 0)

    for c in range(8):

        @pl.when(me != owner_of(c))
        def _():
            first_copy(c).wait_send()
            pltpu.make_async_remote_copy(
                src_ref=ready.at[0],
                dst_ref=out_ref.at[c],
                send_sem=send2.at[0],
                recv_sem=recv2.at[c],
                device_id=place(owner_of(c)),
                device_id_type=MESH,
            ).wait_recv()

    put.wait()
    for dx in range(1, 4):
        weight_copy(dx).wait_send()
        pltpu.make_async_remote_copy(
            src_ref=down_ref.at[:, pl.ds(0, part)],
            dst_ref=mine_rows(lax.rem(x + 4 - dx, 4)),
            send_sem=wsend.at[dx],
            recv_sem=wrecv.at[dx],
            device_id={"tp": lax.rem(x + 4 - dx, 4)},
            device_id_type=MESH,
        ).wait_recv()


def exchange(comp, down):
    n = BLOCK
    depth, part = down.shape[0], down.shape[1] // 4
    return pl.pallas_call(
        exchange_kernel,
        in_specs=[pl.BlockSpec(memory_space=pltpu.VMEM), pl.BlockSpec(memory_space=pl.ANY)],
        out_specs=[pl.BlockSpec(memory_space=pltpu.VMEM), pl.BlockSpec(memory_space=pl.ANY)],
        out_shape=[
            jax.ShapeDtypeStruct((8, n, n), bf16),
            jax.ShapeDtypeStruct((4 * depth, part), bf16),
        ],
        scratch_shapes=[
            pltpu.VMEM((32, n, 2 * n), bf16),
            pltpu.VMEM((32, n, 2 * n), bf16),
            pltpu.VMEM((4, n, 2 * n), f32),
            pltpu.VMEM((4, n, n), bf16),
            pltpu.VMEM((32, n, n), bf16),
            pltpu.VMEM((depth, part), bf16),
            pltpu.SemaphoreType.DMA((8,)),
            pltpu.SemaphoreType.DMA((32,)),
            pltpu.SemaphoreType.DMA((32,)),
            pltpu.SemaphoreType.DMA((8,)),
            pltpu.SemaphoreType.DMA((2,)),
            pltpu.SemaphoreType.DMA((4,)),
            pltpu.SemaphoreType.DMA((4,)),
        ],
        compiler_params=pltpu.CompilerParams(collective_id=0, has_side_effects=True),
        cost_estimate=pl.CostEstimate(flops=9 * 10**9, bytes_accessed=8 * 10**6, transcendentals=0),
        name="exchange",
    )(comp, down)


def finish_kernel(out_ref, qeff_ref, blk_ref, sin_ref, gate_ref, gain_ref, mix_ref):
    n = BLOCK
    gain = gain_ref[...].astype(f32)
    states = {}
    held = [sin_ref[0, d].astype(f32) for d in range(2)]
    for step in range(NBLK):
        for d in range(2):
            b = step if d == 0 else NBLK - 1 - step
            states[d, b] = held[d].astype(bf16)
            if step < NBLK - 1:
                i = d * NBLK + b
                held[d] = mm(blk_ref[0, i, :, n:], states[d, b]) + blk_ref[0, i, :, :n].astype(f32)
    for b in range(NBLK):
        rows = pl.ds(b * n, n)
        both = jnp.concatenate([states[0, b], states[1, b]], axis=0)
        o = out_ref[rows, :] + mm(qeff_ref[0, rows, :], both)
        o = o * lax.rsqrt(jnp.mean(o * o, axis=-1, keepdims=True) + 1e-06) * gain
        g = gate_ref[rows, :].astype(f32)
        mix_ref[rows, :] = (o * (g * jax.nn.sigmoid(g))).astype(bf16)


def finish_pass(out_local, qeff, blk, entering, gates, gain):
    tok, width = out_local.shape
    n = BLOCK
    heads = width // n
    columns = pl.BlockSpec((tok, n), lambda h: (0, h))
    return pl.pallas_call(
        finish_kernel,
        grid=(heads,),
        in_specs=[
            columns,
            pl.BlockSpec((1, tok, 2 * n), lambda h: (h, 0, 0)),
            pl.BlockSpec((1, 2 * NBLK, n, 2 * n), lambda h: (h, 0, 0, 0)),
            pl.BlockSpec((1, 2, n, n), lambda h: (h, 0, 0, 0)),
            columns,
            pl.BlockSpec((1, n), lambda h: (0, 0)),
        ],
        out_specs=columns,
        out_shape=jax.ShapeDtypeStruct((tok, width), bf16),
        compiler_params=ARB,
        name="finish_pass",
    )(out_local, qeff, blk, entering, gates, gain)


def swap_kernel(mix_ref, half_ref, out_ref, other_ref, own_sem, send, recv, wsend, wrecv):
    x = lax.axis_index("tp")
    core = lax.axis_index("sp_2")
    rows, part = mix_ref.shape[0] // 4, mix_ref.shape[1]
    barrier = pltpu.get_barrier_semaphore()
    for dx in range(1, 4):
        pl.semaphore_signal(
            barrier, inc=1, device_id={"tp": lax.rem(x + dx, 4)}, device_id_type=MESH
        )
    pl.semaphore_signal(barrier, inc=1, device_id={"sp_2": 1 - core}, device_id_type=MESH)
    pl.semaphore_wait(barrier, 4)

    few = part // 2

    def rows_of(at, side):
        return mix_ref.at[pl.ds(pl.multiple_of(at * rows, rows), rows), pl.ds(side * few, few)]

    def place_of(half, at, side):
        return out_ref.at[
            pl.ds(half * rows, rows),
            pl.ds(pl.multiple_of(lax.rem(side + core, 2) * 4 * few + at * few, few), few),
        ]

    def copy(half, dx, side, back):
        to = lax.rem(x + (4 - dx if back else dx), 4)
        return pltpu.make_async_remote_copy(
            src_ref=rows_of(lax.rem(to + 2 * half, 4), side),
            dst_ref=place_of(half, lax.rem((to - x if back else x - to) + 4, 4), side),
            send_sem=send.at[half, dx, side], recv_sem=recv.at[half, dx, side],
            device_id={"tp": to}, device_id_type=MESH,
        )

    step = half_ref.shape[0] // 8

    def weight_copy(j):
        rows_j = pl.ds(j * step, step)
        return pltpu.make_async_remote_copy(
            src_ref=half_ref.at[rows_j, :], dst_ref=other_ref.at[rows_j, :],
            send_sem=wsend.at[j], recv_sem=wrecv.at[j], device_id={"sp_2": 1 - core},
            device_id_type=MESH,
        )

    pieces = [(half, side) for half in range(2) for side in range(2)]
    for dx in (2, 1, 3):
        for half, side in pieces:
            copy(half, dx, side, False).start()
    for j in range(8):
        weight_copy(j).start()
    for half, side in pieces:
        own = pltpu.make_async_copy(
            rows_of(lax.rem(x + 2 * half, 4), side),
            place_of(half, 0, side),
            own_sem.at[half, side],
        )
        own.start()
        own.wait()
    for dx in (1, 3, 2):
        for half, side in pieces:
            copy(half, dx, side, False).wait_send()
            copy(half, dx, side, True).wait_recv()
    for j in range(8):
        weight_copy(j).wait()


def swap(mix, half_weight):
    dma = pltpu.SemaphoreType.DMA
    vmem, far_off = (pl.BlockSpec(memory_space=m) for m in (pltpu.VMEM, pl.ANY))
    return pl.pallas_call(
        swap_kernel,
        in_specs=[vmem, far_off],
        out_specs=[vmem, far_off],
        out_shape=[
            jax.ShapeDtypeStruct((mix.shape[0] // 2, mix.shape[1] * 4), bf16),
            jax.ShapeDtypeStruct(half_weight.shape, bf16),
        ],
        scratch_shapes=[dma((2, 2)), dma((2, 4, 2)), dma((2, 4, 2)), dma((8,)), dma((8,))],
        compiler_params=pltpu.CompilerParams(collective_id=3, has_side_effects=True),
        name="swap",
    )(mix, half_weight)


def head_mixing(queries, keys, values, gates, decay_logits, write_logits, extra, rate, gain, down, half_weight):
    tok, width = queries.shape
    heads = width // HEAD_DIM
    log_decay = -rate[:, None, :] * jax.nn.softplus(decay_logits) + extra
    beta = jax.nn.sigmoid(write_logits)

    def per_head(t):
        t = t.transpose(2, 0, 1).reshape(heads, 2 * NBLK, BLOCK)
        return t

    out_local, qeff, blk, comp = local_pass(
        queries, keys, values, per_head(log_decay), per_head(beta), heads
    )
    entering, down_quarter = exchange(comp.reshape(2 * heads, BLOCK, 2 * BLOCK), down)
    mix = finish_pass(
        out_local, qeff, blk, entering.reshape(heads, 2, BLOCK, BLOCK), gates, gain.reshape(1, -1)
    )
    return (*swap(mix, half_weight), down_quarter)


ORDER = (
    (0, 0, 0), (2, 2, 1), (0, 0, 1), (2, 2, 0), (0, 1, 0), (2, 3, 1), (0, 1, 1), (2, 3, 0),
    (1, 0, 0), (2, 1, 1), (1, 0, 1), (2, 1, 0), (0, 3, 0), (3, 2, 1), (0, 3, 1), (3, 2, 0),
    (3, 0, 0), (1, 2, 1), (3, 0, 1), (1, 2, 0), (1, 1, 0), (2, 0, 1), (1, 1, 1), (2, 0, 0),
    (3, 3, 0), (0, 2, 1), (3, 3, 1), (0, 2, 0), (1, 3, 0), (3, 1, 1), (1, 3, 1), (3, 1, 0),
)
CAP = 12
TILE = 512
AHEAD = 8
SLOTS = len(ORDER)
HALF = 2048
FFD = 384
ROWS = SLOTS * CAP


def plane_place(z, y, core, offset, sign):
    dz, dy, dc = offset
    return {
        "sp_0": lax.rem(z + (dz if sign > 0 else 4 - dz), 4),
        "sp_1": lax.rem(y + (dy if sign > 0 else 4 - dy), 4),
        "sp_2": lax.rem(core + dc, 2),
    }


def dispatch_kernel(
    blocks_ref, gate_ref, lin_ref, down_ref, index_ref, weight_ref, stream_ref, out_ref,
    xb, wg, wl, act_buf, hid_ref, wd, ready, back,
    wsem, send0, send1, recv, hsend, rsend, hrecv, hfar, sends, recvs,
):
    z, y, core = (lax.axis_index(a) for a in SP)
    x = lax.axis_index("tp")
    right, left, far = lax.rem(x + 1, 4), lax.rem(x + 3, 4), lax.rem(x + 2, 4)
    keep = pltpu.make_async_copy(blocks_ref.at[0], xb.at[0, 0], wsem.at[2])
    keep.start()
    load_g = pltpu.make_async_copy(gate_ref, wg, wsem.at[0])
    load_l = pltpu.make_async_copy(lin_ref, wl, wsem.at[1])
    load_g.start()
    load_l.start()
    load_d = pltpu.make_async_copy(down_ref, wd, wsem.at[3])
    load_d.start()
    barrier = pltpu.get_barrier_semaphore()
    for dx in range(4):
        for offset in ORDER:
            if dx or offset != ORDER[0]:
                to = plane_place(z, y, core, offset, 1)
                to["tp"] = lax.rem(x + dx, 4)
                pl.semaphore_signal(barrier, inc=1, device_id=to, device_id_type=MESH)
    pl.semaphore_wait(barrier, 4 * SLOTS - 1)

    def plane_copy(i):
        return pltpu.make_async_remote_copy(
            src_ref=blocks_ref.at[i], dst_ref=xb.at[0, i], send_sem=send0.at[i],
            recv_sem=recv.at[0, i], device_id=plane_place(z, y, core, ORDER[i], 1),
            device_id_type=MESH,
        )

    def line_copy(i, to):
        return pltpu.make_async_remote_copy(
            src_ref=xb.at[0, i], dst_ref=xb.at[1, i], send_sem=send1.at[i],
            recv_sem=recv.at[1, i], device_id={"tp": to}, device_id_type=MESH,
        )

    def arrival(pair, i):
        return pltpu.make_async_remote_copy(
            src_ref=blocks_ref.at[0], dst_ref=xb.at[pair, i], send_sem=send0.at[0],
            recv_sem=recv.at[pair, i], device_id={"tp": right}, device_id_type=MESH,
        )

    for i in range(1, AHEAD + 1):
        plane_copy(i).start()
    keep.wait()
    r = lax.broadcasted_iota(jnp.int32, (192, 192), 0)
    c = lax.broadcasted_iota(jnp.int32, (192, 192), 1)
    within = lax.rem(r, 96)
    source = (within // CAP) * (2 * CAP) + (r // 96) * CAP + lax.rem(within, CAP)
    perm = (c == source).astype(f32).astype(bf16)
    source_2 = (lax.rem(r, 2 * CAP) // CAP) * 96 + (r // (2 * CAP)) * CAP + lax.rem(
        lax.rem(r, 2 * CAP), CAP
    )
    perm_2 = (c == source_2).astype(f32).astype(bf16)
    parity = lax.rem(x, 2)
    load_g.wait()
    load_l.wait()
    load_d.wait()

    def compute(pair, part):
        rows = xb[pair, pl.ds(part * 8, 8)].reshape(192, 2 * HALF)
        gate = jnp.minimum(mm(rows, wg[...]), 7.0)
        lin = mm(rows, wl[...])
        act = gate * jax.nn.sigmoid(1.702 * gate) * (jnp.clip(lin, -7.0, 7.0) + 1.0)
        fixed = mm(perm, act.astype(bf16)).astype(bf16)
        low = parity if pair == 0 else 1 - parity
        for half in range(2):
            piece = fixed[half * 96 : (half + 1) * 96]
            act_buf[part, low + 2 * half] = piece
            hid_ref[part, x, low + 2 * half] = piece

    def hid_copy(part, way):
        return pltpu.make_async_remote_copy(
            src_ref=act_buf.at[part], dst_ref=hid_ref.at[part, x],
            send_sem=hsend.at[part, way], recv_sem=hrecv.at[part, x],
            device_id={"tp": lax.rem(x + way, 4)}, device_id_type=MESH,
        )

    def hid_arrival(part, piece):
        return pltpu.make_async_remote_copy(
            src_ref=act_buf.at[part], dst_ref=hid_ref.at[part, piece],
            send_sem=hsend.at[part, 1], recv_sem=hrecv.at[part, piece],
            device_id={"tp": right}, device_id_type=MESH,
        )

    def hid_relay(part, half, piece, to):
        here = hid_ref.at[part, piece, pl.ds(2 * half, 2)]
        return pltpu.make_async_remote_copy(
            src_ref=here, dst_ref=here, send_sem=rsend.at[part, half],
            recv_sem=hfar.at[part, half], device_id={"tp": to}, device_id_type=MESH,
        )

    def relay(part):
        hid_arrival(part, left).wait_recv()
        hid_relay(part, 0, left, right).start()
        hid_arrival(part, right).wait_recv()
        hid_relay(part, 1, right, left).start()

    def send(i, dx):
        to = plane_place(z, y, core, ORDER[i], -1)
        to["tp"] = lax.rem(x + dx, 4)
        return pltpu.make_async_remote_copy(
            src_ref=ready.at[dx, i], dst_ref=back.at[x, i], send_sem=sends.at[dx, i],
            recv_sem=recvs.at[x, i], device_id=to, device_id_type=MESH,
        )

    def project(part):
        totals = []
        for h in range(2):
            cols = pl.ds(h * TILE, TILE)
            total = mm(hid_ref[part, 0].reshape(ROWS, FFD), wd[pl.ds(0, FFD), cols])
            for k in range(1, 4):
                piece = hid_ref[part, k].reshape(ROWS, FFD)
                total = total + mm(piece, wd[pl.ds(k * FFD, FFD), cols])
            totals.append(total.astype(bf16))
        for group in range(4):
            rows = slice(group * 96, (group + 1) * 96)
            both = jnp.concatenate([totals[0][rows], totals[1][rows]], axis=0)
            mixed = mm(perm_2, both).astype(bf16).reshape(8, 2 * CAP, TILE)
            ready[lax.rem(group + 4 - x, 4), pl.ds(part * 8, 8)] = mixed
        for q in range(4):

            @pl.when(part == q)
            def _():
                for i in range(8 * q, 8 * q + 8):
                    for dx in (2, 1, 3, 0):
                        if i or dx:
                            send(i, dx).start()

    def turn(part, carry):
        for p in range(4):

            @pl.when(part == p)
            def _():
                for i in range(8 * p, 8 * p + 8):
                    if i:
                        if i + AHEAD < SLOTS:
                            plane_copy(i).wait_send()
                            plane_copy(i + AHEAD).start()
                        arrival(0, i).wait_recv()
                    line_copy(i, left if i % 2 else right).start()

        @pl.when(part > 0)
        def _():
            relay(part - 1)

        @pl.when(part < 4)
        def _():
            compute(0, part)

            def landed(j, carry):
                arrival(1, part * 8 + j).wait_recv()
                return carry

            lax.fori_loop(0, 8, landed, 0)
            compute(1, part)
            hid_copy(part, 1).start()
            hid_copy(part, 3).start()

        @pl.when(part > 0)
        def _():
            for half in range(2):
                hid_relay(part - 1, half, far, right).wait_recv()
            project(part - 1)

        return carry

    lax.fori_loop(0, 5, turn, 0)
    back[x, 0] = ready[0, 0]
    slots = lax.broadcasted_iota(jnp.int32, (512, SLOTS * 2 * CAP), 1)
    hot = (slots == index_ref[...]).astype(f32).astype(bf16)
    for dx in (0, 1, 3, 2):
        piece = lax.rem(x + dx, 4)
        for i in range(SLOTS):
            if i or dx:
                pltpu.make_async_remote_copy(
                    src_ref=ready.at[0, 0], dst_ref=back.at[piece, i], send_sem=sends.at[0, 0],
                    recv_sem=recvs.at[piece, i], device_id={"tp": right},
                    device_id_type=MESH,
                ).wait_recv()
        arrived = back[piece].reshape(SLOTS * 2 * CAP, TILE)
        for h in range(2):
            cols = pl.ds(pl.multiple_of(piece * (2 * TILE) + h * TILE, TILE), TILE)
            picked = mm(hot[h * 256 : (h + 1) * 256], arrived)
            total = stream_ref[:, cols].astype(f32)
            total = total + picked[:128] * weight_ref[:, 0:1] + picked[128:] * weight_ref[:, 1:2]
            out_ref[:, cols] = total.astype(bf16)

    def finish(part, carry):
        for half in range(2):
            hid_relay(part, half, far, right).wait_send()
        hid_copy(part, 1).wait_send()
        hid_copy(part, 3).wait_send()
        return carry

    lax.fori_loop(0, 4, finish, 0)
    for i in range(SLOTS):
        if i + AHEAD >= SLOTS:
            plane_copy(i).wait_send()
        line_copy(i, right).wait_send()
        for dx in range(4):
            if i or dx:
                send(i, dx).wait_send()


def dispatch(blocks, gate_w, lin_w, down, index, weight, stream):
    width = gate_w.shape[0]
    dma = pltpu.SemaphoreType.DMA
    vmem, far_off = (pl.BlockSpec(memory_space=m) for m in (pltpu.VMEM, pl.ANY))
    return pl.pallas_call(
        dispatch_kernel,
        in_specs=[vmem, far_off, far_off, far_off, vmem, vmem, vmem],
        out_specs=vmem,
        out_shape=jax.ShapeDtypeStruct(stream.shape, bf16),
        scratch_shapes=[
            pltpu.VMEM((2, SLOTS, 2 * CAP, width), bf16),
            pltpu.VMEM((width, FFD), bf16),
            pltpu.VMEM((width, FFD), bf16),
            pltpu.VMEM((4, 4, 96, FFD), bf16),
            pltpu.VMEM((4, 4, 4, 96, FFD), bf16),
            pltpu.VMEM(down.shape, bf16),
            pltpu.VMEM((4, SLOTS, 2 * CAP, TILE), bf16),
            pltpu.VMEM((4, SLOTS, 2 * CAP, TILE), bf16),
            dma((4,)), dma((SLOTS,)), dma((SLOTS,)), dma((2, SLOTS)),
            dma((4, 4)), dma((4, 2)), dma((4, 4)), dma((4, 2)), dma((4, SLOTS)), dma((4, SLOTS)),
        ],
        compiler_params=pltpu.CompilerParams(
            collective_id=1, has_side_effects=True, vmem_limit_bytes=58 * 1024 * 1024
        ),
        name="experts",
    )(blocks, gate_w, lin_w, down, index, weight, stream)


def slot_table(selected):
    z, y, core = (lax.axis_index(a) for a in SP)
    count = selected.shape[0]
    flat = selected.reshape(-1)
    member = (flat[:, None] == jnp.arange(SLOTS, dtype=jnp.int32)[None, :]).astype(jnp.int32)
    rank = jnp.sum(jnp.cumsum(member, axis=0) * member, axis=1) - 1
    away_z = (flat // 8 - z) % 4
    away_y = (flat // 2 % 4 - y) % 4
    away = (away_z * 4 + away_y) * 2 + (flat - core) % 2
    slot = jnp.zeros_like(flat)
    for i, (dz, dy, dc) in enumerate(ORDER):
        slot = slot + jnp.where(away == (dz * 4 + dy) * 2 + dc, i, 0)
    return slot.reshape(count, TOPK), rank.reshape(count, TOPK)


def expert_layer(stream, normed, selected, other, route_weight, gate_w, lin_w, down_quarter):
    rows = selected.shape[0]
    late = lax.axis_index("tp") // 2
    slot, rank = slot_table(selected)
    first = slot * (2 * CAP) + rank
    table = jnp.stack([first.T, first.T + CAP])
    slot_2, rank_2 = slot_table(other)
    source = jnp.concatenate(
        [first + late * CAP, slot_2 * (2 * CAP) + rank_2 + (1 - late) * CAP], axis=0
    )
    slots = jnp.arange(SLOTS * 2 * CAP, dtype=jnp.int32)[:, None]
    hot = (slots == source[None, :, 0]).astype(bf16) + (slots == source[None, :, 1]).astype(bf16)
    blocks = jnp.dot(hot, normed, preferred_element_type=f32).astype(bf16)
    return dispatch(
        blocks.reshape(SLOTS, 2 * CAP, 2 * HALF),
        gate_w,
        lin_w,
        down_quarter,
        table.reshape(4 * rows, 1),
        route_weight,
        stream,
    )


def per_device(
    queries,
    keys,
    values,
    output_gate_logits,
    decay_gate_logits,
    write_strength_logits,
    extra_log_decay,
    head_decay_rate,
    head_norm_gain,
    output_weight,
    residual,
    expert_norm_gain,
    selected_experts,
    router_chosen_scores,
    gate_up_weight,
    linear_up_weight,
    down_weight,
):
    core = lax.axis_index("sp_2")
    place = lax.axis_index("sp_0") * 4 + lax.axis_index("sp_1")
    few = output_weight.shape[0] // lax.axis_size(SP)
    first_row = core * (output_weight.shape[0] // 2) + place * few
    own_rows = lax.dynamic_slice_in_dim(output_weight, first_row, few, axis=0)
    line = [own_rows] + [
        lax.ppermute(own_rows, "tp", [(i, (i - dx) % 4) for i in range(4)]) for dx in range(1, 4)
    ]
    half_weight = lax.all_gather(jnp.stack(line), ("sp_0", "sp_1"), axis=1, tiled=True)
    half_weight = half_weight.reshape(-1, output_weight.shape[1])
    opposite = [(i, (i + 2) % 4) for i in range(4)]
    residual_2 = lax.ppermute(residual, "tp", opposite)
    selected_2 = lax.ppermute(selected_experts, "tp", opposite)
    head_mix, other_weight, down_quarter = head_mixing(
        queries,
        keys,
        values,
        output_gate_logits,
        decay_gate_logits,
        write_strength_logits,
        extra_log_decay,
        head_decay_rate,
        head_norm_gain,
        down_weight[0],
        half_weight,
    )
    split = half_weight.shape[0]
    mix_sum = jnp.dot(head_mix[:, :split], half_weight, preferred_element_type=jnp.float32)
    mix_sum = mix_sum + jnp.dot(
        head_mix[:, split:], other_weight, preferred_element_type=jnp.float32
    )
    both = jnp.concatenate([residual, residual_2], axis=0)
    stream = (both.astype(jnp.float32) + mix_sum).astype(jnp.bfloat16)
    stream_wide = stream.astype(jnp.float32)
    normed = (
        stream_wide
        * lax.rsqrt(jnp.mean(stream_wide * stream_wide, axis=-1, keepdims=True) + 1e-06)
        * expert_norm_gain.astype(jnp.float32)
    ).astype(jnp.bfloat16)
    route_exp = jnp.exp(router_chosen_scores)
    route_weight = route_exp / jnp.sum(route_exp, axis=-1, keepdims=True)
    return expert_layer(
        stream[: residual.shape[0]],
        normed,
        selected_experts,
        selected_2,
        route_weight,
        gate_up_weight[0],
        linear_up_weight[0],
        down_quarter,
    )


def solution(mesh):
    torus = Mesh(mesh.devices.reshape(4, 4, 2, mesh.shape["tp"]), ("sp_0", "sp_1", "sp_2", "tp"))
    placed = (
        P(SP, "tp"),
        P(SP, "tp"),
        P(SP, "tp"),
        P(SP, "tp"),
        P(None, SP, "tp"),
        P(None, SP, "tp"),
        P(None, SP, "tp"),
        P(None, "tp"),
        P(),
        P("tp", None),
        P(SP_TP, None),
        P(),
        P(SP_TP, None),
        P(SP_TP, None),
        P(SP, None, "tp"),
        P(SP, None, "tp"),
        P(SP, "tp", None),
    )
    return jax.shard_map(
        per_device, mesh=torus, in_specs=placed, out_specs=P(SP_TP, None), check_vma=False
    )
```

```python
import jax
import jax.numpy as jnp
from jax import lax
from jax.experimental import pallas as pl
from jax.experimental.pallas import tpu as pltpu
from jax.sharding import Mesh
from jax.sharding import PartitionSpec as P

HEAD_DIM = 128
TOPK = 2
BLOCK = 128
SP = ("sp_0", "sp_1", "sp_2")
SP_TP = ("sp_0", "sp_1", "sp_2", "tp")
ARB = pltpu.CompilerParams(dimension_semantics=("arbitrary",), vmem_limit_bytes=48 * 1024 * 1024)
MESH = pl.DeviceIdType.MESH
NBLK = 4
f32 = jnp.float32
bf16 = jnp.bfloat16


def mm(a, b):
    return jnp.dot(a, b, preferred_element_type=f32)


def local_kernel(q_ref, k_ref, v_ref, ld_ref, bt_ref, out_ref, qeff_ref, blk_ref, comp_ref):
    n = BLOCK
    row = lax.broadcasted_iota(jnp.int32, (n, n), 0)
    col = lax.broadcasted_iota(jnp.int32, (n, n), 1)
    upper = (row <= col).astype(f32)
    lower = (row >= col).astype(f32)
    eye = (row == col).astype(f32)
    ld = ld_ref[0]
    highest = lax.Precision.HIGHEST
    run_f = jnp.dot(ld, upper, precision=highest, preferred_element_type=f32)
    run_b = jnp.dot(ld, lower, precision=highest, preferred_element_type=f32)
    which = lax.broadcasted_iota(jnp.int32, (2 * NBLK, n), 0)
    cum_rows = jnp.where(which < NBLK, run_f, run_b)
    cum_cols = jnp.transpose(cum_rows)
    beta_cols = jnp.transpose(bt_ref[0])
    chains = [(d, b) for d in range(2) for b in range(NBLK)]
    grams, k_un, v_un, q_un, kt_un = [], [], [], [], []
    for b in range(NBLK):
        rows = pl.ds(b * n, n)
        q = q_ref[rows, :].astype(f32)
        k = k_ref[rows, :].astype(f32)
        q = q * lax.rsqrt(jnp.sum(q * q, axis=-1, keepdims=True) + 1e-06) * HEAD_DIM ** (-0.5)
        k = k * lax.rsqrt(jnp.sum(k * k, axis=-1, keepdims=True) + 1e-06)
        kt = jnp.transpose(k).astype(bf16)
        grams.append((mm(k.astype(bf16), kt), mm(q.astype(bf16), kt)))
        q_un.append(q)
        k_un.append(k)
        kt_un.append(kt)
        v_un.append(v_ref[rows, :].astype(f32))
    low, attn, sums, pows = {}, {}, {}, {}
    for d, b in chains:
        i = d * NBLK + b
        gap = cum_cols[:, i : i + 1] - cum_rows[i : i + 1, :]
        keep = row >= col if d == 0 else row <= col
        decay = jnp.exp(jnp.where(keep, gap, -1e30))
        attn[d, b] = (grams[b][1] * decay).astype(bf16)
        strict = row > col if d == 0 else row < col
        low = jnp.where(strict, grams[b][0] * decay, 0.0) * beta_cols[:, i : i + 1]
        sums[d, b] = eye - low
        pows[d, b] = low.astype(bf16)
    for c in chains:
        pows[c] = mm(pows[c], pows[c]).astype(bf16)
    for step in range(5):
        for c in chains:
            both = mm(jnp.concatenate([sums[c].astype(bf16), pows[c]], axis=0), pows[c])
            sums[c] = sums[c] + both[:n]
            pows[c] = both[n:].astype(bf16)
    for c in chains:
        sums[c] = sums[c] + mm(sums[c].astype(bf16), pows[c])
    fresh, maps = {}, {}
    for d, b in chains:
        i = d * NBLK + b
        cc = cum_cols[:, i : i + 1]
        bt = beta_cols[:, i : i + 1]
        right = jnp.concatenate([v_un[b] * bt, k_un[b] * (-bt * jnp.exp(cc))], axis=1)
        fresh[d, b] = mm(sums[d, b].astype(bf16), right.astype(bf16))
    for d, b in chains:
        i = d * NBLK + b
        cc = cum_cols[:, i : i + 1]
        last = n - 1 if d == 0 else 0
        total = cum_rows[i : i + 1, last : last + 1]
        ended = (fresh[d, b] * jnp.exp(total - cc)).astype(bf16)
        step_map = mm(kt_un[b], ended) + jnp.concatenate(
            [jnp.zeros((n, n), f32), eye * jnp.exp(total)], axis=1
        )
        maps[d, b] = step_map
        blk_ref[0, i] = step_map.astype(bf16)
    for b in range(NBLK):
        rows = pl.ds(b * n, n)
        locals_, effs = [], []
        for d in range(2):
            i = d * NBLK + b
            given = mm(attn[d, b], fresh[d, b].astype(bf16))
            locals_.append(given[:, :n])
            effs.append(given[:, n:] + q_un[b] * jnp.exp(cum_cols[:, i : i + 1]))
        out_ref[rows, :] = locals_[0] + locals_[1]
        qeff_ref[0, rows, :] = jnp.concatenate(effs, axis=1).astype(bf16)

    def after(later, earlier):
        moved = mm(later[:, n:].astype(bf16), earlier.astype(bf16))
        return jnp.concatenate([moved[:, :n] + later[:, :n], moved[:, n:]], axis=1)

    for d in range(2):
        order = range(NBLK) if d == 0 else range(NBLK - 1, -1, -1)
        first, second, third, fourth = [maps[d, b] for b in order]
        comp_ref[0, d] = after(after(fourth, third), after(second, first)).astype(bf16)


def local_pass(queries, keys, values, log_decay, beta, heads):
    tok = queries.shape[0]
    n = BLOCK
    columns = pl.BlockSpec((tok, n), lambda h: (0, h))
    small = pl.BlockSpec((1, 2 * NBLK, n), lambda h: (h, 0, 0))
    return pl.pallas_call(
        local_kernel,
        grid=(heads,),
        in_specs=[columns, columns, columns, small, small],
        out_specs=[
            columns,
            pl.BlockSpec((1, tok, 2 * n), lambda h: (h, 0, 0)),
            pl.BlockSpec((1, 2 * NBLK, n, 2 * n), lambda h: (h, 0, 0, 0)),
            pl.BlockSpec((1, 2, n, 2 * n), lambda h: (h, 0, 0, 0)),
        ],
        out_shape=[
            jax.ShapeDtypeStruct((tok, heads * n), f32),
            jax.ShapeDtypeStruct((heads, tok, 2 * n), bf16),
            jax.ShapeDtypeStruct((heads, 2 * NBLK, n, 2 * n), bf16),
            jax.ShapeDtypeStruct((heads, 2, n, 2 * n), bf16),
        ],
        compiler_params=ARB,
        cost_estimate=pl.CostEstimate(flops=4 * 10**9, bytes_accessed=8 * 10**6, transcendentals=0),
        name="local_pass",
    )(queries, keys, values, log_decay, beta)


def exchange_kernel(
    comp_ref, down_ref, out_ref, quarter_ref,
    got, pre, chunk, start, ready, held_w, send1, recv1, send2, recv2, wsem, wsend, wrecv,
):
    n = BLOCK
    z, y, core = (lax.axis_index(a) for a in SP)
    x = lax.axis_index("tp")
    me = (z * 4 + y) * 2 + core
    depth, part = down_ref.shape[0], down_ref.shape[1] // 4
    take = pltpu.make_async_copy(
        down_ref.at[:, pl.ds(pl.multiple_of(x * part, part), part)], held_w, wsem.at[0]
    )
    take.start()
    is_owner = jnp.logical_and(core == 1, y % 2 == z % 2)
    way = y // 2
    mine = z * 2 + way

    def place(s):
        return {"sp_0": s // 8, "sp_1": (s // 2) % 4, "sp_2": s % 2}

    barrier = pltpu.get_barrier_semaphore()

    def greet(i, carry):
        other = (me + i) % 32
        pl.semaphore_signal(barrier, inc=1, device_id=place(other), device_id_type=MESH)
        return carry

    lax.fori_loop(1, 32, greet, 0)
    for dx in range(1, 4):
        pl.semaphore_signal(
            barrier, inc=1, device_id={"tp": lax.rem(x + dx, 4)}, device_id_type=MESH
        )
    pl.semaphore_wait(barrier, 34)

    def owner_of(c):
        oz = c // 2
        return (oz * 4 + (c % 2) * 2 + oz % 2) * 2 + 1

    def first_copy(c):
        return pltpu.make_async_remote_copy(
            src_ref=comp_ref.at[c],
            dst_ref=got.at[me],
            send_sem=send1.at[c],
            recv_sem=recv1.at[me],
            device_id=place(owner_of(c)),
            device_id_type=MESH,
        )

    for c in range(8):
        own = owner_of(c)

        @pl.when(me != own)
        def _():
            first_copy(c).start()

        @pl.when(me == own)
        def _():
            got[me] = comp_ref[c]

    def mine_rows(at):
        return quarter_ref.at[pl.ds(pl.multiple_of(at * depth, depth), depth), :]

    def weight_copy(dx):
        to = lax.rem(x + dx, 4)
        return pltpu.make_async_remote_copy(
            src_ref=down_ref.at[:, pl.ds(pl.multiple_of(to * part, part), part)],
            dst_ref=mine_rows(x),
            send_sem=wsend.at[dx],
            recv_sem=wrecv.at[dx],
            device_id={"tp": to},
            device_id_type=MESH,
        )

    for dx in range(1, 4):
        weight_copy(dx).start()
    take.wait()
    put = pltpu.make_async_copy(held_w, mine_rows(x), wsem.at[1])
    put.start()

    def arrival(s):
        return pltpu.make_async_remote_copy(
            src_ref=comp_ref.at[0],
            dst_ref=got.at[s],
            send_sem=send1.at[0],
            recv_sem=recv1.at[s],
            device_id=place(s),
            device_id_type=MESH,
        )

    def second_copy(p, s):
        return pltpu.make_async_remote_copy(
            src_ref=ready.at[p],
            dst_ref=out_ref.at[mine],
            send_sem=send2.at[p],
            recv_sem=recv2.at[mine],
            device_id=place(s),
            device_id_type=MESH,
        )

    @pl.when(is_owner)
    def _():
        row = lax.broadcasted_iota(jnp.int32, (n, 2 * n), 0)
        col = lax.broadcasted_iota(jnp.int32, (n, 2 * n), 1)
        unit = (row + n == col).astype(f32)
        for j in range(4):
            chunk[j] = unit

        def step(r, carry):
            for j in range(4):
                p = 8 * j + r
                s = p + way * (31 - 2 * p)

                @pl.when(s != me)
                def _():
                    arrival(s).wait_recv()

                now = chunk[j].astype(bf16)
                pre[p] = now
                moved = mm(got[s, :, n:], now)
                chunk[j, :, :n] = moved[:, :n] + got[s, :, :n].astype(f32)
                chunk[j, :, n:] = moved[:, n:]
            return carry

        lax.fori_loop(0, 8, step, 0)
        start[0] = jnp.zeros((n, n), bf16)
        held = jnp.zeros((n, n), f32)
        for j in range(3):
            held = mm(chunk[j, :, n:].astype(bf16), held.astype(bf16)) + chunk[j, :, :n]
            start[j + 1] = held.astype(bf16)

        def finish(r, carry):
            for j in range(4):
                p = 8 * j + r
                s = p + way * (31 - 2 * p)
                given = mm(pre[p, :, n:], start[j]) + pre[p, :, :n].astype(f32)
                ready[p] = given.astype(bf16)

                @pl.when(s != me)
                def _():
                    second_copy(p, s).start()

                @pl.when(s == me)
                def _():
                    out_ref[mine] = given.astype(bf16)

            return carry

        lax.fori_loop(0, 8, finish, 0)

        def drain(p, carry):
            s = p + way * (31 - 2 * p)

            @pl.when(s != me)
            def _():
                second_copy(p, s).wait_send()

            return carry

        lax.fori_loop(0, 32, drain, 0)

    for c in range(8):

        @pl.when(me != owner_of(c))
        def _():
            first_copy(c).wait_send()
            pltpu.make_async_remote_copy(
                src_ref=ready.at[0],
                dst_ref=out_ref.at[c],
                send_sem=send2.at[0],
                recv_sem=recv2.at[c],
                device_id=place(owner_of(c)),
                device_id_type=MESH,
            ).wait_recv()

    put.wait()
    for dx in range(1, 4):
        weight_copy(dx).wait_send()
        pltpu.make_async_remote_copy(
            src_ref=down_ref.at[:, pl.ds(0, part)],
            dst_ref=mine_rows(lax.rem(x + 4 - dx, 4)),
            send_sem=wsend.at[dx],
            recv_sem=wrecv.at[dx],
            device_id={"tp": lax.rem(x + 4 - dx, 4)},
            device_id_type=MESH,
        ).wait_recv()


def exchange(comp, down):
    n = BLOCK
    depth, part = down.shape[0], down.shape[1] // 4
    return pl.pallas_call(
        exchange_kernel,
        in_specs=[pl.BlockSpec(memory_space=pltpu.VMEM), pl.BlockSpec(memory_space=pl.ANY)],
        out_specs=[pl.BlockSpec(memory_space=pltpu.VMEM), pl.BlockSpec(memory_space=pl.ANY)],
        out_shape=[
            jax.ShapeDtypeStruct((8, n, n), bf16),
            jax.ShapeDtypeStruct((4 * depth, part), bf16),
        ],
        scratch_shapes=[
            pltpu.VMEM((32, n, 2 * n), bf16),
            pltpu.VMEM((32, n, 2 * n), bf16),
            pltpu.VMEM((4, n, 2 * n), f32),
            pltpu.VMEM((4, n, n), bf16),
            pltpu.VMEM((32, n, n), bf16),
            pltpu.VMEM((depth, part), bf16),
            pltpu.SemaphoreType.DMA((8,)),
            pltpu.SemaphoreType.DMA((32,)),
            pltpu.SemaphoreType.DMA((32,)),
            pltpu.SemaphoreType.DMA((8,)),
            pltpu.SemaphoreType.DMA((2,)),
            pltpu.SemaphoreType.DMA((4,)),
            pltpu.SemaphoreType.DMA((4,)),
        ],
        compiler_params=pltpu.CompilerParams(collective_id=0, has_side_effects=True),
        cost_estimate=pl.CostEstimate(flops=9 * 10**9, bytes_accessed=8 * 10**6, transcendentals=0),
        name="exchange",
    )(comp, down)


def finish_kernel(out_ref, qeff_ref, blk_ref, sin_ref, gate_ref, gain_ref, mix_ref):
    n = BLOCK
    gain = gain_ref[...].astype(f32)
    states = {}
    held = [sin_ref[0, d].astype(f32) for d in range(2)]
    for step in range(NBLK):
        for d in range(2):
            b = step if d == 0 else NBLK - 1 - step
            states[d, b] = held[d].astype(bf16)
            if step < NBLK - 1:
                i = d * NBLK + b
                held[d] = mm(blk_ref[0, i, :, n:], states[d, b]) + blk_ref[0, i, :, :n].astype(f32)
    for b in range(NBLK):
        rows = pl.ds(b * n, n)
        both = jnp.concatenate([states[0, b], states[1, b]], axis=0)
        o = out_ref[rows, :] + mm(qeff_ref[0, rows, :], both)
        o = o * lax.rsqrt(jnp.mean(o * o, axis=-1, keepdims=True) + 1e-06) * gain
        g = gate_ref[rows, :].astype(f32)
        mix_ref[rows, :] = (o * (g * jax.nn.sigmoid(g))).astype(bf16)


def finish_pass(out_local, qeff, blk, entering, gates, gain):
    tok, width = out_local.shape
    n = BLOCK
    heads = width // n
    columns = pl.BlockSpec((tok, n), lambda h: (0, h))
    return pl.pallas_call(
        finish_kernel,
        grid=(heads,),
        in_specs=[
            columns,
            pl.BlockSpec((1, tok, 2 * n), lambda h: (h, 0, 0)),
            pl.BlockSpec((1, 2 * NBLK, n, 2 * n), lambda h: (h, 0, 0, 0)),
            pl.BlockSpec((1, 2, n, n), lambda h: (h, 0, 0, 0)),
            columns,
            pl.BlockSpec((1, n), lambda h: (0, 0)),
        ],
        out_specs=columns,
        out_shape=jax.ShapeDtypeStruct((tok, width), bf16),
        compiler_params=ARB,
        name="finish_pass",
    )(out_local, qeff, blk, entering, gates, gain)


def swap_kernel(mix_ref, half_ref, out_ref, other_ref, own_sem, send, recv, wsend, wrecv):
    x = lax.axis_index("tp")
    core = lax.axis_index("sp_2")
    rows, part = mix_ref.shape[0] // 4, mix_ref.shape[1]
    barrier = pltpu.get_barrier_semaphore()
    for dx in range(1, 4):
        pl.semaphore_signal(
            barrier, inc=1, device_id={"tp": lax.rem(x + dx, 4)}, device_id_type=MESH
        )
    pl.semaphore_signal(barrier, inc=1, device_id={"sp_2": 1 - core}, device_id_type=MESH)
    pl.semaphore_wait(barrier, 4)

    few = part // 2

    def rows_of(at, side):
        return mix_ref.at[pl.ds(pl.multiple_of(at * rows, rows), rows), pl.ds(side * few, few)]

    def place_of(half, at, side):
        return out_ref.at[
            pl.ds(half * rows, rows),
            pl.ds(pl.multiple_of(lax.rem(side + core, 2) * 4 * few + at * few, few), few),
        ]

    def copy(half, dx, side, back):
        to = lax.rem(x + (4 - dx if back else dx), 4)
        return pltpu.make_async_remote_copy(
            src_ref=rows_of(lax.rem(to + 2 * half, 4), side),
            dst_ref=place_of(half, lax.rem((to - x if back else x - to) + 4, 4), side),
            send_sem=send.at[half, dx, side], recv_sem=recv.at[half, dx, side],
            device_id={"tp": to}, device_id_type=MESH,
        )

    step = half_ref.shape[0] // 8

    def weight_copy(j):
        rows_j = pl.ds(j * step, step)
        return pltpu.make_async_remote_copy(
            src_ref=half_ref.at[rows_j, :], dst_ref=other_ref.at[rows_j, :],
            send_sem=wsend.at[j], recv_sem=wrecv.at[j], device_id={"sp_2": 1 - core},
            device_id_type=MESH,
        )

    pieces = [(half, side) for half in range(2) for side in range(2)]
    for dx in (2, 1, 3):
        for half, side in pieces:
            copy(half, dx, side, False).start()
    for j in range(8):
        weight_copy(j).start()
    for half, side in pieces:
        own = pltpu.make_async_copy(
            rows_of(lax.rem(x + 2 * half, 4), side),
            place_of(half, 0, side),
            own_sem.at[half, side],
        )
        own.start()
        own.wait()
    for dx in (1, 3, 2):
        for half, side in pieces:
            copy(half, dx, side, False).wait_send()
            copy(half, dx, side, True).wait_recv()
    for j in range(8):
        weight_copy(j).wait()


def swap(mix, half_weight):
    dma = pltpu.SemaphoreType.DMA
    vmem, far_off = (pl.BlockSpec(memory_space=m) for m in (pltpu.VMEM, pl.ANY))
    return pl.pallas_call(
        swap_kernel,
        in_specs=[vmem, far_off],
        out_specs=[vmem, far_off],
        out_shape=[
            jax.ShapeDtypeStruct((mix.shape[0] // 2, mix.shape[1] * 4), bf16),
            jax.ShapeDtypeStruct(half_weight.shape, bf16),
        ],
        scratch_shapes=[dma((2, 2)), dma((2, 4, 2)), dma((2, 4, 2)), dma((8,)), dma((8,))],
        compiler_params=pltpu.CompilerParams(collective_id=3, has_side_effects=True),
        name="swap",
    )(mix, half_weight)


def head_mixing(queries, keys, values, gates, decay_logits, write_logits, extra, rate, gain, down, half_weight):
    tok, width = queries.shape
    heads = width // HEAD_DIM
    log_decay = -rate[:, None, :] * jax.nn.softplus(decay_logits) + extra
    beta = jax.nn.sigmoid(write_logits)

    def per_head(t):
        t = t.transpose(2, 0, 1).reshape(heads, 2 * NBLK, BLOCK)
        return t

    out_local, qeff, blk, comp = local_pass(
        queries, keys, values, per_head(log_decay), per_head(beta), heads
    )
    entering, down_quarter = exchange(comp.reshape(2 * heads, BLOCK, 2 * BLOCK), down)
    mix = finish_pass(
        out_local, qeff, blk, entering.reshape(heads, 2, BLOCK, BLOCK), gates, gain.reshape(1, -1)
    )
    return (*swap(mix, half_weight), down_quarter)


ORDER = (
    (0, 0, 0), (2, 2, 1), (0, 0, 1), (2, 2, 0), (0, 1, 0), (2, 3, 1), (0, 1, 1), (2, 3, 0),
    (1, 0, 0), (2, 1, 1), (1, 0, 1), (2, 1, 0), (0, 3, 0), (3, 2, 1), (0, 3, 1), (3, 2, 0),
    (3, 0, 0), (1, 2, 1), (3, 0, 1), (1, 2, 0), (1, 1, 0), (2, 0, 1), (1, 1, 1), (2, 0, 0),
    (3, 3, 0), (0, 2, 1), (3, 3, 1), (0, 2, 0), (1, 3, 0), (3, 1, 1), (1, 3, 1), (3, 1, 0),
)
CAP = 12
TILE = 512
AHEAD = 12
SLOTS = len(ORDER)
HALF = 2048
FFD = 384
ROWS = SLOTS * CAP


def plane_place(z, y, core, offset, sign):
    dz, dy, dc = offset
    return {
        "sp_0": lax.rem(z + (dz if sign > 0 else 4 - dz), 4),
        "sp_1": lax.rem(y + (dy if sign > 0 else 4 - dy), 4),
        "sp_2": lax.rem(core + dc, 2),
    }


def dispatch_kernel(
    blocks_ref, gate_ref, lin_ref, down_ref, index_ref, weight_ref, stream_ref, out_ref,
    xb, wg, wl, act_buf, hid_ref, wd, ready, back,
    wsem, send0, send1, recv, hsend, rsend, hrecv, hfar, sends, recvs,
):
    z, y, core = (lax.axis_index(a) for a in SP)
    x = lax.axis_index("tp")
    right, left, far = lax.rem(x + 1, 4), lax.rem(x + 3, 4), lax.rem(x + 2, 4)
    keep = pltpu.make_async_copy(blocks_ref.at[0], xb.at[0, 0], wsem.at[2])
    keep.start()
    load_g = pltpu.make_async_copy(gate_ref, wg, wsem.at[0])
    load_l = pltpu.make_async_copy(lin_ref, wl, wsem.at[1])
    load_g.start()
    load_l.start()
    load_d = pltpu.make_async_copy(down_ref, wd, wsem.at[3])
    load_d.start()
    barrier = pltpu.get_barrier_semaphore()
    for dx in range(4):
        for offset in ORDER:
            if dx or offset != ORDER[0]:
                to = plane_place(z, y, core, offset, 1)
                to["tp"] = lax.rem(x + dx, 4)
                pl.semaphore_signal(barrier, inc=1, device_id=to, device_id_type=MESH)
    pl.semaphore_wait(barrier, 4 * SLOTS - 1)

    def plane_copy(i):
        return pltpu.make_async_remote_copy(
            src_ref=blocks_ref.at[i], dst_ref=xb.at[0, i], send_sem=send0.at[i],
            recv_sem=recv.at[0, i], device_id=plane_place(z, y, core, ORDER[i], 1),
            device_id_type=MESH,
        )

    def line_copy(i, to):
        return pltpu.make_async_remote_copy(
            src_ref=xb.at[0, i], dst_ref=xb.at[1, i], send_sem=send1.at[i],
            recv_sem=recv.at[1, i], device_id={"tp": to}, device_id_type=MESH,
        )

    def arrival(pair, i):
        return pltpu.make_async_remote_copy(
            src_ref=blocks_ref.at[0], dst_ref=xb.at[pair, i], send_sem=send0.at[0],
            recv_sem=recv.at[pair, i], device_id={"tp": right}, device_id_type=MESH,
        )

    for i in range(1, AHEAD + 1):
        plane_copy(i).start()
    keep.wait()
    r = lax.broadcasted_iota(jnp.int32, (192, 192), 0)
    c = lax.broadcasted_iota(jnp.int32, (192, 192), 1)
    within = lax.rem(r, 96)
    source = (within // CAP) * (2 * CAP) + (r // 96) * CAP + lax.rem(within, CAP)
    perm = (c == source).astype(f32).astype(bf16)
    source_2 = (lax.rem(r, 2 * CAP) // CAP) * 96 + (r // (2 * CAP)) * CAP + lax.rem(
        lax.rem(r, 2 * CAP), CAP
    )
    perm_2 = (c == source_2).astype(f32).astype(bf16)
    parity = lax.rem(x, 2)
    load_g.wait()
    load_l.wait()
    load_d.wait()

    def compute(pair, part):
        rows = xb[pair, pl.ds(part * 8, 8)].reshape(192, 2 * HALF)
        gate = jnp.minimum(mm(rows, wg[...]), 7.0)
        lin = mm(rows, wl[...])
        act = gate * jax.nn.sigmoid(1.702 * gate) * (jnp.clip(lin, -7.0, 7.0) + 1.0)
        fixed = mm(perm, act.astype(bf16)).astype(bf16)
        low = parity if pair == 0 else 1 - parity
        for half in range(2):
            piece = fixed[half * 96 : (half + 1) * 96]
            act_buf[part, low + 2 * half] = piece
            hid_ref[part, x, low + 2 * half] = piece

    def hid_copy(part, way):
        return pltpu.make_async_remote_copy(
            src_ref=act_buf.at[part], dst_ref=hid_ref.at[part, x],
            send_sem=hsend.at[part, way], recv_sem=hrecv.at[part, x],
            device_id={"tp": lax.rem(x + way, 4)}, device_id_type=MESH,
        )

    def hid_arrival(part, piece):
        return pltpu.make_async_remote_copy(
            src_ref=act_buf.at[part], dst_ref=hid_ref.at[part, piece],
            send_sem=hsend.at[part, 1], recv_sem=hrecv.at[part, piece],
            device_id={"tp": right}, device_id_type=MESH,
        )

    def hid_relay(part, half, piece, to):
        here = hid_ref.at[part, piece, pl.ds(2 * half, 2)]
        return pltpu.make_async_remote_copy(
            src_ref=here, dst_ref=here, send_sem=rsend.at[part, half],
            recv_sem=hfar.at[part, half], device_id={"tp": to}, device_id_type=MESH,
        )

    def relay(part):
        hid_arrival(part, left).wait_recv()
        hid_relay(part, 0, left, right).start()
        hid_arrival(part, right).wait_recv()
        hid_relay(part, 1, right, left).start()

    def send(i, dx):
        to = plane_place(z, y, core, ORDER[i], -1)
        to["tp"] = lax.rem(x + dx, 4)
        return pltpu.make_async_remote_copy(
            src_ref=ready.at[dx, i], dst_ref=back.at[x, i], send_sem=sends.at[dx, i],
            recv_sem=recvs.at[x, i], device_id=to, device_id_type=MESH,
        )

    def project(part):
        totals = []
        for h in range(2):
            cols = pl.ds(h * TILE, TILE)
            total = mm(hid_ref[part, 0].reshape(ROWS, FFD), wd[pl.ds(0, FFD), cols])
            for k in range(1, 4):
                piece = hid_ref[part, k].reshape(ROWS, FFD)
                total = total + mm(piece, wd[pl.ds(k * FFD, FFD), cols])
            totals.append(total.astype(bf16))
        for group in range(4):
            rows = slice(group * 96, (group + 1) * 96)
            both = jnp.concatenate([totals[0][rows], totals[1][rows]], axis=0)
            mixed = mm(perm_2, both).astype(bf16).reshape(8, 2 * CAP, TILE)
            ready[lax.rem(group + 4 - x, 4), pl.ds(part * 8, 8)] = mixed
        for q in range(4):

            @pl.when(part == q)
            def _():
                for i in range(8 * q, 8 * q + 8):
                    for dx in (2, 1, 3, 0):
                        if i or dx:
                            send(i, dx).start()

    def turn(part, carry):
        for p in range(4):

            @pl.when(part == p)
            def _():
                for i in range(8 * p, 8 * p + 8):
                    if i:
                        if i + AHEAD < SLOTS:
                            plane_copy(i).wait_send()
                            plane_copy(i + AHEAD).start()
                        arrival(0, i).wait_recv()
                    line_copy(i, left if i % 2 else right).start()

        @pl.when(part > 0)
        def _():
            relay(part - 1)

        @pl.when(part < 4)
        def _():
            compute(0, part)

            def landed(j, carry):
                arrival(1, part * 8 + j).wait_recv()
                return carry

            lax.fori_loop(0, 8, landed, 0)
            compute(1, part)
            hid_copy(part, 1).start()
            hid_copy(part, 3).start()

        @pl.when(part > 0)
        def _():
            for half in range(2):
                hid_relay(part - 1, half, far, right).wait_recv()
            project(part - 1)

        return carry

    lax.fori_loop(0, 5, turn, 0)
    back[x, 0] = ready[0, 0]
    slots = lax.broadcasted_iota(jnp.int32, (512, SLOTS * 2 * CAP), 1)
    hot = (slots == index_ref[...]).astype(f32).astype(bf16)
    for dx in (0, 1, 3, 2):
        piece = lax.rem(x + dx, 4)
        for i in range(SLOTS):
            if i or dx:
                pltpu.make_async_remote_copy(
                    src_ref=ready.at[0, 0], dst_ref=back.at[piece, i], send_sem=sends.at[0, 0],
                    recv_sem=recvs.at[piece, i], device_id={"tp": right},
                    device_id_type=MESH,
                ).wait_recv()
        arrived = back[piece].reshape(SLOTS * 2 * CAP, TILE)
        for h in range(2):
            cols = pl.ds(pl.multiple_of(piece * (2 * TILE) + h * TILE, TILE), TILE)
            picked = mm(hot[h * 256 : (h + 1) * 256], arrived)
            total = stream_ref[:, cols].astype(f32)
            total = total + picked[:128] * weight_ref[:, 0:1] + picked[128:] * weight_ref[:, 1:2]
            out_ref[:, cols] = total.astype(bf16)

    def finish(part, carry):
        for half in range(2):
            hid_relay(part, half, far, right).wait_send()
        hid_copy(part, 1).wait_send()
        hid_copy(part, 3).wait_send()
        return carry

    lax.fori_loop(0, 4, finish, 0)
    for i in range(SLOTS):
        if i + AHEAD >= SLOTS:
            plane_copy(i).wait_send()
        line_copy(i, right).wait_send()
        for dx in range(4):
            if i or dx:
                send(i, dx).wait_send()


def dispatch(blocks, gate_w, lin_w, down, index, weight, stream):
    width = gate_w.shape[0]
    dma = pltpu.SemaphoreType.DMA
    vmem, far_off = (pl.BlockSpec(memory_space=m) for m in (pltpu.VMEM, pl.ANY))
    return pl.pallas_call(
        dispatch_kernel,
        in_specs=[vmem, far_off, far_off, far_off, vmem, vmem, vmem],
        out_specs=vmem,
        out_shape=jax.ShapeDtypeStruct(stream.shape, bf16),
        scratch_shapes=[
            pltpu.VMEM((2, SLOTS, 2 * CAP, width), bf16),
            pltpu.VMEM((width, FFD), bf16),
            pltpu.VMEM((width, FFD), bf16),
            pltpu.VMEM((4, 4, 96, FFD), bf16),
            pltpu.VMEM((4, 4, 4, 96, FFD), bf16),
            pltpu.VMEM(down.shape, bf16),
            pltpu.VMEM((4, SLOTS, 2 * CAP, TILE), bf16),
            pltpu.VMEM((4, SLOTS, 2 * CAP, TILE), bf16),
            dma((4,)), dma((SLOTS,)), dma((SLOTS,)), dma((2, SLOTS)),
            dma((4, 4)), dma((4, 2)), dma((4, 4)), dma((4, 2)), dma((4, SLOTS)), dma((4, SLOTS)),
        ],
        compiler_params=pltpu.CompilerParams(
            collective_id=1, has_side_effects=True, vmem_limit_bytes=58 * 1024 * 1024
        ),
        name="experts",
    )(blocks, gate_w, lin_w, down, index, weight, stream)


def slot_table(selected):
    z, y, core = (lax.axis_index(a) for a in SP)
    count = selected.shape[0]
    flat = selected.reshape(-1)
    member = (flat[:, None] == jnp.arange(SLOTS, dtype=jnp.int32)[None, :]).astype(jnp.int32)
    rank = jnp.sum(jnp.cumsum(member, axis=0) * member, axis=1) - 1
    away_z = (flat // 8 - z) % 4
    away_y = (flat // 2 % 4 - y) % 4
    away = (away_z * 4 + away_y) * 2 + (flat - core) % 2
    slot = jnp.zeros_like(flat)
    for i, (dz, dy, dc) in enumerate(ORDER):
        slot = slot + jnp.where(away == (dz * 4 + dy) * 2 + dc, i, 0)
    return slot.reshape(count, TOPK), rank.reshape(count, TOPK)


def expert_layer(stream, normed, selected, other, route_weight, gate_w, lin_w, down_quarter):
    rows = selected.shape[0]
    late = lax.axis_index("tp") // 2
    slot, rank = slot_table(selected)
    first = slot * (2 * CAP) + rank
    table = jnp.stack([first.T, first.T + CAP])
    slot_2, rank_2 = slot_table(other)
    source = jnp.concatenate(
        [first + late * CAP, slot_2 * (2 * CAP) + rank_2 + (1 - late) * CAP], axis=0
    )
    slots = jnp.arange(SLOTS * 2 * CAP, dtype=jnp.int32)[:, None]
    hot = (slots == source[None, :, 0]).astype(bf16) + (slots == source[None, :, 1]).astype(bf16)
    blocks = jnp.dot(hot, normed, preferred_element_type=f32).astype(bf16)
    return dispatch(
        blocks.reshape(SLOTS, 2 * CAP, 2 * HALF),
        gate_w,
        lin_w,
        down_quarter,
        table.reshape(4 * rows, 1),
        route_weight,
        stream,
    )


def per_device(
    queries,
    keys,
    values,
    output_gate_logits,
    decay_gate_logits,
    write_strength_logits,
    extra_log_decay,
    head_decay_rate,
    head_norm_gain,
    output_weight,
    residual,
    expert_norm_gain,
    selected_experts,
    router_chosen_scores,
    gate_up_weight,
    linear_up_weight,
    down_weight,
):
    core = lax.axis_index("sp_2")
    place = lax.axis_index("sp_0") * 4 + lax.axis_index("sp_1")
    few = output_weight.shape[0] // lax.axis_size(SP)
    first_row = core * (output_weight.shape[0] // 2) + place * few
    own_rows = lax.dynamic_slice_in_dim(output_weight, first_row, few, axis=0)
    line = [own_rows] + [
        lax.ppermute(own_rows, "tp", [(i, (i - dx) % 4) for i in range(4)]) for dx in range(1, 4)
    ]
    half_weight = lax.all_gather(jnp.stack(line), ("sp_0", "sp_1"), axis=1, tiled=True)
    half_weight = half_weight.reshape(-1, output_weight.shape[1])
    opposite = [(i, (i + 2) % 4) for i in range(4)]
    residual_2 = lax.ppermute(residual, "tp", opposite)
    selected_2 = lax.ppermute(selected_experts, "tp", opposite)
    head_mix, other_weight, down_quarter = head_mixing(
        queries,
        keys,
        values,
        output_gate_logits,
        decay_gate_logits,
        write_strength_logits,
        extra_log_decay,
        head_decay_rate,
        head_norm_gain,
        down_weight[0],
        half_weight,
    )
    split = half_weight.shape[0]
    mix_sum = jnp.dot(head_mix[:, :split], half_weight, preferred_element_type=jnp.float32)
    mix_sum = mix_sum + jnp.dot(
        head_mix[:, split:], other_weight, preferred_element_type=jnp.float32
    )
    both = jnp.concatenate([residual, residual_2], axis=0)
    stream = (both.astype(jnp.float32) + mix_sum).astype(jnp.bfloat16)
    stream_wide = stream.astype(jnp.float32)
    normed = (
        stream_wide
        * lax.rsqrt(jnp.mean(stream_wide * stream_wide, axis=-1, keepdims=True) + 1e-06)
        * expert_norm_gain.astype(jnp.float32)
    ).astype(jnp.bfloat16)
    route_exp = jnp.exp(router_chosen_scores)
    route_weight = route_exp / jnp.sum(route_exp, axis=-1, keepdims=True)
    return expert_layer(
        stream[: residual.shape[0]],
        normed,
        selected_experts,
        selected_2,
        route_weight,
        gate_up_weight[0],
        linear_up_weight[0],
        down_quarter,
    )


def solution(mesh):
    torus = Mesh(mesh.devices.reshape(4, 4, 2, mesh.shape["tp"]), ("sp_0", "sp_1", "sp_2", "tp"))
    placed = (
        P(SP, "tp"),
        P(SP, "tp"),
        P(SP, "tp"),
        P(SP, "tp"),
        P(None, SP, "tp"),
        P(None, SP, "tp"),
        P(None, SP, "tp"),
        P(None, "tp"),
        P(),
        P("tp", None),
        P(SP_TP, None),
        P(),
        P(SP_TP, None),
        P(SP_TP, None),
        P(SP, None, "tp"),
        P(SP, None, "tp"),
        P(SP, "tp", None),
    )
    return jax.shard_map(
        per_device, mesh=torus, in_specs=placed, out_specs=P(SP_TP, None), check_vma=False
    )
```
